32 devices in a mesh: grp: 2 (over y), sp: 4 (over z), tp: 4 (over x, core).
Axes of the slice: x: 2, y: 2, z: 4, core: 2. Of those that a mesh axis runs over, the one named last changes fastest.
Arguments:
- query_wide: bfloat16 [4096, 1024], P(('grp', 'sp'), 'tp'), parts along dimension 0, may hold values from -6 to 6
- key_wide: bfloat16 [4096, 1024], P(('grp', 'sp'), 'tp'), parts along dimension 0, may hold values from -6 to 6
- value_wide: bfloat16 [4096, 1024], P(('grp', 'sp'), 'tp'), parts along dimension 0, may hold values from -6 to 6
- decay_wide: float32 [4096, 8], P(('grp', 'sp'), 'tp'), parts along dimension 0, may hold values from -2 to 0, as said below
- query_narrow: bfloat16 [4096, 1024], P(('grp', 'sp'), 'tp'), parts along dimension 0, may hold values from -6 to 6
- key_narrow: bfloat16 [4096, 1024], P(('grp', 'sp'), 'tp'), parts along dimension 0, may hold values from -6 to 6
- value_narrow: bfloat16 [4096, 1024], P(('grp', 'sp'), 'tp'), parts along dimension 0, may hold values from -6 to 6
- decay_narrow: float32 [4096, 16], P(('grp', 'sp'), 'tp'), parts along dimension 0, may hold values from -2 to 0, as said below
- residual: bfloat16 [4096, 2048], P(('grp', 'sp', 'tp')), parts along dimension 0, may hold values from -6 to 6
- out_wide: bfloat16 [1024, 2048], P('tp'), may hold values from -0.125 to 0.125
- out_narrow: bfloat16 [1024, 2048], P('tp'), may hold values from -0.125 to 0.125
- norm_gain: float32 [2048], replicated, may hold values from 0.1 to 1.9
- routes: int32 [4096, 2], P(('grp', 'sp', 'tp')), parts along dimension 0, may hold values from 0 to 3, all different within a row; in each aligned block of 128 rows (0 to 127, 128 to 255, ...) at most 96 rows name the same one
- route_weights: float32 [4096, 2], P(('grp', 'sp', 'tp')), parts along dimension 0, may hold values from 0.1 to 1
- expert_gate: bfloat16 [4, 2048, 2048], P('sp', None, 'tp'), may hold values from -0.375 to 0.375
- expert_up: bfloat16 [4, 2048, 2048], P('sp', None, 'tp'), may hold values from -0.375 to 0.375
- expert_down: bfloat16 [4, 2048, 2048], P('sp', 'tp'), may hold values from -0.03125 to 0.03125
Outputs:
- layer_out: bfloat16 [4096, 2048], P(('grp', 'sp', 'tp')), parts along dimension 0
The draws below stay inside these ranges and needn't reach their ends.
There are 2 independent parts, one for each index of `grp`. The reference program is written for one: setup_inputs(seed, part) draws one part's arguments, and reference() takes and returns one part's arrays. A program takes and returns all parts, laid end to end along the dimension named above; an argument that names none is the same for every part. Nothing has to cross between parts.
Inputs may be any that keep to these rules, and one draw needn't show every extreme that they name: `decay_wide`: every entry is negative. `decay_narrow`: every entry is negative. `routes`: each row names 2 different experts; on the rows of one device no expert is named more than 96 times, a bound that some block reaches.
All inputs are finite; a program needn't handle non-finite values.
Results may differ from the reference program's by a relative error of at most 0.018.
Values may be sent and summed in bfloat16 or wider, within the bound.
A program may use at most 128 MiB of HBM per device.

```python
import math
import jax
import jax.numpy as jnp
import numpy as np
from jax import lax

D = 2048
HEADS_WIDE = 8
HEAD_WIDE = 128
HEADS_NARROW = 16
HEAD_NARROW = 64
FF = 2048
TOP_K = 2
TOK_DEV = 512
STEP_COUNT_FULL = 2048
EXPERTS = 4
ROWS_DEV = 128
CAPACITY = 96
N_SP = 4
N_TP = 4


def decay_draw(key, attention_group_count):
    lookup_vectors = jax.random.split(key, 7)
    fast_share = 0.5
    fast_heads = jax.random.uniform(lookup_vectors[0], (attention_group_count,), jnp.float32) < fast_share
    fast_rate = jax.random.uniform(lookup_vectors[1], (attention_group_count,), jnp.float32, 1.0 / 50.0, 1.0 / 20.0)
    slow_rate = jax.random.uniform(lookup_vectors[2], (attention_group_count,), jnp.float32, 0.1, 0.4) / STEP_COUNT_FULL
    ground_frequency = jnp.where(fast_heads, fast_rate, slow_rate)
    block_count = STEP_COUNT_FULL // TOK_DEV
    block_factor = jnp.exp(jax.random.uniform(lookup_vectors[3], (block_count, attention_group_count), jnp.float32, -0.7, 0.7))
    place_indices = jnp.repeat(block_factor, TOK_DEV, axis=0)
    noise_amplitude = jax.random.uniform(lookup_vectors[4], (STEP_COUNT_FULL, attention_group_count), jnp.float32, 0.5, 1.5)
    spike_place = jax.random.randint(lookup_vectors[5], (2,), 0, STEP_COUNT_FULL)
    spike_magnitude = jax.random.uniform(lookup_vectors[6], (2, attention_group_count), jnp.float32, 0.22, 0.69)
    spike_entry_indices = (jnp.arange(STEP_COUNT_FULL)[:, None] == spike_place[None, :]).astype(jnp.float32)
    return -(ground_frequency[None, :] * place_indices * noise_amplitude) - jnp.dot(spike_entry_indices, spike_magnitude)


def draw_decay_wide(key, part):
    return decay_draw(jax.random.fold_in(key, 11), HEADS_WIDE)


def draw_decay_narrow(key, part):
    return decay_draw(jax.random.fold_in(key, 23), HEADS_NARROW)


def level_of(rng, extent, shards, least, largest):
    loudness, own = 1.0, jax.random.fold_in(rng, 6)
    for position, parts in shards:
        draws = jnp.exp(jax.random.uniform(jax.random.fold_in(own, position), (parts,), jnp.float32, least / len(shards), largest / len(shards)))
        loudness = loudness * jnp.repeat(draws, extent[position] // parts).reshape([-1 if axis == position else 1 for axis in range(len(extent))])
    return loudness


def deal_out(own_key, own, number, rows, number_of, top, most, lean):
    order = jax.random.permutation(own_key, number_of)
    crowded, usual = load_shares(number_of, rows * top, most, lean, True), load_shares(number_of, rows * top, most, lean, False)
    places = jnp.arange(number_of)

    def named(lengths, offset_by):
        used = int((lengths > 0).sum())
        fixed = max(1, used // 4)
        shifted = fixed + (places - fixed + offset_by * (used - fixed)) % max(1, number_of - fixed)
        return jnp.zeros((number_of,), jnp.int32).at[order[jnp.where(places < fixed, places, shifted)]].set(jnp.asarray(lengths, jnp.int32))

    lengths = jnp.where(number % 4 == 0, named(crowded, number // 4), named(usual, number - number // 4 - 1))
    mixed = jax.random.permutation(jax.random.fold_in(own, 3), number_of)
    donor, taker = mixed[0:number_of // 2 * 2:2], mixed[1:number_of // 2 * 2:2]
    room = jnp.minimum(lengths[donor] - 1, most - lengths[taker]) // 2
    room = jnp.where((donor == order[0]) | (taker == order[0]) | (lengths[taker] == 0), 0, jnp.maximum(room, 0))
    shifted = jax.random.randint(jax.random.fold_in(own, 4), (number_of // 2,), 0, 1 << 20) % (room + 1)
    lengths = lengths.at[donor].add(-shifted).at[taker].add(shifted)
    members = jnp.searchsorted(jnp.cumsum(lengths), jnp.arange(rows * top), side="right").astype(jnp.int32)
    table = members.reshape(top, rows).T
    table = table[jax.random.permutation(jax.random.fold_in(own, 1), rows)]
    offset_by = jax.random.randint(jax.random.fold_in(own, 2), (rows, 1), 0, top)
    return jnp.take_along_axis(table, (jnp.arange(top)[None, :] + offset_by) % top, axis=1)


def load_shares(amount, total, limit, slope, full):
    weights = [(1 << 20) // math.isqrt(grade ** slope) + 1 for grade in range(1, amount + 1)]
    largest = limit if full else min(limit, max(-(-total // amount), total * weights[0] // sum(weights)))
    least = 1 if total - largest >= amount - 1 else 0
    counts, rest = [largest] + [least] * (amount - 1), total - largest - least * (amount - 1)
    while rest > 0:
        free = [i for i in range(1, amount) if counts[i] < largest] or [i for i in range(1, amount) if counts[i] < limit]
        pool, remaining = sum([weights[i] for i in free]), rest
        for i in free:
            extra = min(limit - counts[i], max(1, remaining * weights[i] // pool), rest)
            counts[i] = counts[i] + extra
            rest = rest - extra
    return np.array(counts)


def noise(key, shape, width, reach, cuts=(), kind=jnp.bfloat16):
    result = jax.random.normal(key, shape, jnp.float32) * width
    if len(cuts) > 0:
        result = level_of(key, shape, cuts, -0.22, 0.18) * result
    return jnp.clip(result, min=-reach, max=reach).astype(kind)


def setup_inputs(seed: int = 0, part: int = 0) -> dict:
    arg_keys = jax.random.split(jax.random.key(seed), 18)
    part_splits = jax.random.split(jax.random.fold_in(arg_keys[17], part), 18)
    query_wide = noise(part_splits[0], (STEP_COUNT_FULL, HEADS_WIDE * HEAD_WIDE), 1.0, 6.0, ((0, 4), (1, 4)))
    key_wide = noise(part_splits[1], (STEP_COUNT_FULL, HEADS_WIDE * HEAD_WIDE), 1.0, 6.0, ((0, 4), (1, 4)))
    value_wide = noise(part_splits[2], (STEP_COUNT_FULL, HEADS_WIDE * HEAD_WIDE), 1.0, 6.0, ((0, 4), (1, 4)))
    decay_wide = draw_decay_wide(jax.random.fold_in(jax.random.fold_in(arg_keys[17], part), 71), part)
    query_narrow = noise(part_splits[4], (STEP_COUNT_FULL, HEADS_NARROW * HEAD_NARROW), 1.0, 6.0, ((0, 4), (1, 4)))
    key_narrow = noise(part_splits[5], (STEP_COUNT_FULL, HEADS_NARROW * HEAD_NARROW), 1.0, 6.0, ((0, 4), (1, 4)))
    value_narrow = noise(part_splits[6], (STEP_COUNT_FULL, HEADS_NARROW * HEAD_NARROW), 1.0, 6.0, ((0, 4), (1, 4)))
    decay_narrow = draw_decay_narrow(jax.random.fold_in(jax.random.fold_in(arg_keys[17], part), 71), part)
    residual = noise(part_splits[8], (STEP_COUNT_FULL, D), 1.0, 6.0, ((0, 16),))
    out_wide = noise(arg_keys[9], (HEADS_WIDE * HEAD_WIDE, D), (HEADS_WIDE * HEAD_WIDE + HEADS_NARROW * HEAD_NARROW) ** -0.5, 0.125, ((0, 4),))
    out_narrow = noise(arg_keys[10], (HEADS_NARROW * HEAD_NARROW, D), (HEADS_WIDE * HEAD_WIDE + HEADS_NARROW * HEAD_NARROW) ** -0.5, 0.125, ((0, 4),))
    norm_gain = jnp.clip(1.0 + 0.18 * jax.random.normal(arg_keys[11], (D,), jnp.float32), 0.1, 1.9)
    routes_keys = jax.random.split(jax.random.fold_in(part_splits[12], 1), STEP_COUNT_FULL // ROWS_DEV)
    routes_turns = jax.random.permutation(jax.random.fold_in(part_splits[12], 3), STEP_COUNT_FULL // ROWS_DEV)
    routes = jax.vmap(lambda own, number: deal_out(jax.random.fold_in(part_splits[12], 2), own, number, ROWS_DEV, EXPERTS, TOP_K, CAPACITY, 1))(routes_keys, routes_turns).reshape((STEP_COUNT_FULL, TOP_K))
    route_weights = jnp.clip(jnp.exp(math.log(1.0) - 2.3025851 * jax.random.uniform(part_splits[13], (STEP_COUNT_FULL, TOP_K), jnp.float32) ** level_of(part_splits[13], (STEP_COUNT_FULL, TOP_K), ((0, 16),), -0.2, 0.2)), 0.1, 1.0)
    expert_gate = noise(arg_keys[14], (EXPERTS, D, FF), (D // 9) ** -0.5, 0.375, ((0, 4), (2, 4)))
    expert_up = noise(arg_keys[15], (EXPERTS, D, FF), (D // 9) ** -0.5, 0.375, ((0, 4), (2, 4)))
    expert_down = noise(arg_keys[16], (EXPERTS, FF, D), (FF * 16) ** -0.5, 0.03125, ((0, 4), (1, 4)))
    return {"query_wide": query_wide, "key_wide": key_wide, "value_wide": value_wide, "decay_wide": decay_wide, "query_narrow": query_narrow, "key_narrow": key_narrow, "value_narrow": value_narrow, "decay_narrow": decay_narrow, "residual": residual, "out_wide": out_wide, "out_narrow": out_narrow, "norm_gain": norm_gain, "routes": routes, "route_weights": route_weights, "expert_gate": expert_gate, "expert_up": expert_up, "expert_down": expert_down}


norm_eps = 1e-05
clamp_limit = 7.0
swish_alpha = 1.702
rotary_base = 10000.0
highest = lax.Precision.HIGHEST

def rotate(values, positions):
    half_width = values.shape[-1] // 2
    inverse = rotary_base ** (-jnp.arange(half_width, dtype=jnp.float32) / half_width)
    angles = positions[:, None] * inverse[None, :]
    cosine = jnp.cos(angles)[:, None, :]
    sine_part = jnp.sin(angles)[:, None, :]
    lower_half = values[..., :half_width]
    upper_half = values[..., half_width:]
    return jnp.concatenate([lower_half * cosine - upper_half * sine_part, lower_half * sine_part + upper_half * cosine], axis=-1)

def prepare(query_in, key_in, head_width, positions):
    length = query_in.shape[0]
    attention_group_count = query_in.shape[1] // head_width
    query_heads = query_in.astype(jnp.float32).reshape(length, attention_group_count, head_width)
    key_heads = key_in.astype(jnp.float32).reshape(length, attention_group_count, head_width)
    query_rot = rotate(query_heads, positions).astype(jnp.bfloat16)
    key_rot = (rotate(key_heads, positions) * head_width ** (-0.5)).astype(jnp.bfloat16)
    return (query_rot, key_rot)

def group_norm(output_heads):
    center = lax.optimization_barrier(jnp.mean(output_heads, axis=-1, keepdims=True))
    spread = lax.optimization_barrier(jnp.mean(jnp.square(output_heads - center), axis=-1, keepdims=True))
    return (output_heads - center) * lax.rsqrt(spread + norm_eps)

def block_terms(query_f, key_f, value_f, log_decay):
    block_len = query_f.shape[0]
    cumulative = jnp.cumsum(log_decay, axis=0)
    steps_in = jnp.arange(block_len, dtype=jnp.int32)
    causal = steps_in[:, None] >= steps_in[None, :]
    gaps = cumulative.T[:, :, None] - cumulative.T[:, None, :]
    decay_grid = jnp.exp(jnp.where(causal[None], gaps, -jnp.inf))
    scores = jnp.einsum('thd,shd->hts', query_f, key_f, precision=highest) * decay_grid
    inner_part = jnp.einsum('hts,she->the', scores, value_f, precision=highest)
    total_log = cumulative[-1]
    weighted = key_f * jnp.exp(total_log[None, :] - cumulative)[:, :, None]
    state_local = jnp.einsum('shd,she->hde', weighted, value_f, precision=highest)
    return (inner_part, cumulative, total_log, state_local)

def read_carried(query_f, cumulative, state_in):
    return jnp.exp(cumulative)[:, :, None] * jnp.einsum('thd,hde->the', query_f, state_in, precision=highest)

def retain(query_in, key_in, value_in, log_decay, head_width):
    length = query_in.shape[0]
    attention_group_count = query_in.shape[1] // head_width
    positions = jnp.arange(length, dtype=jnp.float32)
    query_rot, key_rot = prepare(query_in, key_in, head_width, positions)
    block_len = math.gcd(length, 128)
    blocks = length // block_len

    def advance(state_now, inputs):
        query_block, key_block, value_block, decay_block = inputs
        query_f = query_block.astype(jnp.float32)
        key_f = key_block.astype(jnp.float32)
        value_f = value_block.astype(jnp.float32)
        inner_part, cumulative, total_log, state_local = block_terms(query_f, key_f, value_f, decay_block)
        output_block = inner_part + read_carried(query_f, cumulative, state_now)
        state_next = jnp.exp(total_log)[:, None, None] * state_now + state_local
        return (state_next, output_block)
    value_heads = value_in.reshape(length, attention_group_count, head_width)
    inputs = (query_rot.reshape(blocks, block_len, attention_group_count, head_width), key_rot.reshape(blocks, block_len, attention_group_count, head_width), value_heads.reshape(blocks, block_len, attention_group_count, head_width), log_decay.reshape(blocks, block_len, attention_group_count))
    final_state, outputs = lax.scan(advance, jnp.zeros((attention_group_count, head_width, head_width), jnp.float32), inputs)
    normed_heads = group_norm(outputs.reshape(length, attention_group_count, head_width))
    return normed_heads.reshape(length, attention_group_count * head_width).astype(jnp.bfloat16)

def activate(gate_pre, up_pre):
    gate_clip = jnp.minimum(gate_pre, clamp_limit)
    up_clip = jnp.clip(up_pre, -clamp_limit, clamp_limit)
    return gate_clip * jax.nn.sigmoid(swish_alpha * gate_clip) * (up_clip + 1.0)

def round_trip(values):
    return lax.optimization_barrier(values.astype(jnp.bfloat16)).astype(jnp.float32)

def moe_reference(normed, routes, route_weights, expert_gate, expert_up, expert_down):
    length = normed.shape[0]
    slot_count = N_SP * N_TP * CAPACITY
    padded = jnp.concatenate([normed, jnp.zeros((1, D), jnp.bfloat16)], axis=0)

    def per_expert(total_rows, inputs):
        expert_index, gate_w, up_w, down_w = inputs
        chosen = routes == expert_index
        hits = jnp.any(chosen, axis=1).astype(jnp.int32)
        weight = lax.optimization_barrier(jnp.sum(jnp.where(chosen, route_weights, 0.0), axis=1))
        weight_pad = jnp.concatenate([weight, jnp.zeros((1,), jnp.float32)])
        rank_in = jnp.cumsum(hits) - hits
        target = jnp.where(hits > 0, rank_in, slot_count).astype(jnp.int32)
        slot_table = jnp.full((slot_count + 1,), length, jnp.int32).at[target].set(jnp.arange(length, dtype=jnp.int32))[:slot_count]
        slot_rows = padded[slot_table]
        gate_pre = jnp.dot(slot_rows, gate_w, preferred_element_type=jnp.float32)
        up_pre = jnp.dot(slot_rows, up_w, preferred_element_type=jnp.float32)
        hidden = activate(gate_pre, up_pre).astype(jnp.bfloat16)
        pieces = hidden.reshape(slot_count, N_TP, FF // N_TP).astype(jnp.float32)
        down_parts = down_w.reshape(N_TP, FF // N_TP, D).astype(jnp.float32)
        partial_value = jnp.einsum('nqf,qfd->qnd', pieces, down_parts)
        summed = lax.optimization_barrier(jnp.sum(round_trip(partial_value), axis=0))
        expert_output = summed.astype(jnp.bfloat16).astype(jnp.float32)
        contrib = expert_output * weight_pad[slot_table][:, None]
        return (total_rows.at[slot_table].add(contrib), None)
    total_rows, unused = lax.scan(per_expert, jnp.zeros((length + 1, D), jnp.float32), (jnp.arange(EXPERTS, dtype=jnp.int32), expert_gate, expert_up, expert_down))
    return total_rows[:length]

def reference(query_wide, key_wide, value_wide, decay_wide, query_narrow, key_narrow, value_narrow, decay_narrow, residual, out_wide, out_narrow, norm_gain, routes, route_weights, expert_gate, expert_up, expert_down):
    mixed_wide = retain(query_wide, key_wide, value_wide, decay_wide, HEAD_WIDE)
    mixed_narrow = retain(query_narrow, key_narrow, value_narrow, decay_narrow, HEAD_NARROW)
    wide_share = HEADS_WIDE * HEAD_WIDE // N_TP
    narrow_share = HEADS_NARROW * HEAD_NARROW // N_TP
    attention = jnp.zeros((STEP_COUNT_FULL, D), jnp.float32)
    for tp_part in range(N_TP):
        wide_cols = slice(tp_part * wide_share, (tp_part + 1) * wide_share)
        narrow_cols = slice(tp_part * narrow_share, (tp_part + 1) * narrow_share)
        partial_value = jnp.dot(mixed_wide[:, wide_cols], out_wide[wide_cols], preferred_element_type=jnp.float32)
        partial_value = partial_value + jnp.dot(mixed_narrow[:, narrow_cols], out_narrow[narrow_cols], preferred_element_type=jnp.float32)
        attention = attention + round_trip(partial_value)
    hidden_state = residual.astype(jnp.float32) + attention
    scale_row = lax.rsqrt(lax.optimization_barrier(jnp.mean(hidden_state * hidden_state, axis=-1, keepdims=True)) + norm_eps)
    normed = (hidden_state * scale_row * norm_gain).astype(jnp.bfloat16)
    routed = moe_reference(normed, routes, route_weights, expert_gate, expert_up, expert_down)
    return (hidden_state + routed).astype(jnp.bfloat16)
```

```python
import functools

import jax
import jax.numpy as jnp
import numpy as np
from jax import lax
from jax.experimental import pallas as pl
from jax.experimental.pallas import tpu as pltpu
from jax.sharding import PartitionSpec as P

HEAD_WIDE = 128
HEAD_NARROW = 64
TOP_K = 2


norm_eps = 1e-05
clamp_limit = 7.0
swish_alpha = 1.702
rotary_base = 10000.0


def activate(gate_pre, up_pre):
    gate_clip = jnp.minimum(gate_pre, clamp_limit)
    up_clip = jnp.clip(up_pre, -clamp_limit, clamp_limit)
    return gate_clip * jax.nn.sigmoid(swish_alpha * gate_clip) * (up_clip + 1.0)


MESH = pl.DeviceIdType.MESH


def tail_kernel(
    experts,
    capacity,
    queries_hbm,
    queries_narrow_hbm,
    keys_hbm,
    keys_narrow_hbm,
    values_hbm,
    values_narrow_hbm,
    out_wide_hbm,
    out_narrow_hbm,
    residual_hbm,
    gate_hbm,
    up_hbm,
    down_hbm,
    decay_wide,
    decay_narrow,
    coarse,
    fine,
    gain,
    routes,
    weights,
    output,
    mixer_in,
    outs_in,
    residual,
    gate,
    up,
    down,
    decays,
    log_rows,
    log_columns,
    turns,
    slot_rows,
    slot_columns,
    weight_columns,
    part,
    part_in,
    cross,
    cross_in,
    hidden_state,
    send,
    rows,
    result,
    result_in,
    half,
    half_in,
    summed,
    returned,
    mixed,
    inner,
    turned,
    local_state,
    local_total,
    states,
    totals,
    load_sem,
    s_send,
    s_recv,
    t_send,
    t_recv,
    a_send,
    a_recv,
    z_send,
    z_recv,
    x_send,
    x_recv,
    p_send,
    p_recv,
    c_send,
    c_recv,
    h_send,
    h_recv,
    r_send,
    r_recv,
):
    place = lax.axis_index("sp")
    mine = lax.axis_index("tp")
    core, side = mine % 2, mine // 2
    partner = side * 2 + (1 - core)
    across = (1 - side) * 2 + core
    model_width = residual.shape[1]

    def remote(src, dst, send_sem, recv_sem, **where):
        return pltpu.make_async_remote_copy(
            src_ref=src,
            dst_ref=dst,
            send_sem=send_sem,
            recv_sem=recv_sem,
            device_id=where,
            device_id_type=MESH,
        )

    def peer(step):
        return lax.rem(place + step, experts) if experts & (experts - 1) else place ^ step

    sources = (
        (keys_hbm, mixer_in.at[2]),
        (keys_narrow_hbm, mixer_in.at[3]),
        (values_hbm, mixer_in.at[4]),
        (values_narrow_hbm, mixer_in.at[5]),
        (queries_hbm, mixer_in.at[0]),
        (queries_narrow_hbm, mixer_in.at[1]),
        (out_wide_hbm, outs_in.at[0]),
        (out_narrow_hbm, outs_in.at[1]),
        (residual_hbm, residual),
        (gate_hbm, gate),
        (up_hbm, up),
        (down_hbm, down),
    )
    every_load = [
        pltpu.make_async_copy(src, dst, load_sem.at[n]) for n, (src, dst) in enumerate(sources)
    ]
    for load in every_load:
        load.start()
    loads = every_load[9:]
    queries, queries_narrow = mixer_in.at[0], mixer_in.at[1]
    keys, keys_narrow = mixer_in.at[2], mixer_in.at[3]
    values, values_narrow = mixer_in.at[4], mixer_in.at[5]
    out_wide, out_narrow = outs_in.at[0], outs_in.at[1]

    barrier = pltpu.get_barrier_semaphore()
    pl.semaphore_signal(barrier, inc=1, device_id={"tp": partner}, device_id_type=MESH)
    pl.semaphore_signal(barrier, inc=1, device_id={"tp": across}, device_id_type=MESH)

    @pl.loop(1, experts)
    def _(step):
        pl.semaphore_signal(barrier, inc=1, device_id={"sp": peer(step)}, device_id_type=MESH)

    length = queries.shape[0]
    rows_dev = residual.shape[0]
    fine_rows = fine.shape[2]
    coarse_rows = length // fine_rows
    at_coarse = pl.multiple_of(place * coarse_rows, coarse_rows)
    for narrow in range(2):
        cosine_fine, sine_fine = fine[narrow, 0], fine[narrow, 1]
        cosine_coarse = coarse[narrow, 0, pl.ds(at_coarse, coarse_rows), :]
        sine_coarse = coarse[narrow, 1, pl.ds(at_coarse, coarse_rows), :]
        for at in range(coarse_rows):
            cosine, sine_part = cosine_coarse[at : at + 1], sine_coarse[at : at + 1]
            span = slice(at * fine_rows, (at + 1) * fine_rows)
            turns[narrow, 0, span] = cosine * cosine_fine - sine_part * sine_fine
            turns[narrow, 1, span] = sine_part * cosine_fine + cosine * sine_fine

    def pieces_of(value):
        high = value.astype(jnp.bfloat16)
        rest = value - high.astype(jnp.float32)
        middle = rest.astype(jnp.bfloat16)
        low = (rest - middle.astype(jnp.float32)).astype(jnp.bfloat16)
        return high, middle, low

    row_at = lax.broadcasted_iota(jnp.int32, (128, 128), 0)
    lane_at = lax.broadcasted_iota(jnp.int32, (128, 128), 1)
    up_to = (row_at <= lane_at).astype(jnp.bfloat16)
    heads_wide, heads_narrow = decay_wide.shape[0], decay_narrow.shape[0]
    decays[...] = jnp.zeros_like(decays)
    decays[0:heads_wide, :] = decay_wide[...]
    decays[heads_wide : heads_wide + heads_narrow, :] = decay_narrow[...]
    running = jnp.zeros((8, 1), jnp.float32)
    for at in range(0, length, 128):
        within = running
        for piece in pieces_of(decays[:, at : at + 128]):
            within = within + jnp.dot(piece, up_to, preferred_element_type=jnp.float32)
        log_rows[:, at : at + 128] = within
        log_columns[at : at + 128, :] = within.T
        running = within[:, 127:128]

    named = lax.broadcasted_iota(jnp.int32, (slot_rows.shape[0], rows_dev), 0)
    hits = (routes[0:1, :] == named) | (routes[1:2, :] == named)
    earlier = lax.broadcasted_iota(jnp.int32, (rows_dev, rows_dev), 0) < lax.broadcasted_iota(
        jnp.int32, (rows_dev, rows_dev), 1
    )
    rank = jnp.dot(
        hits.astype(jnp.bfloat16),
        earlier.astype(jnp.bfloat16),
        preferred_element_type=jnp.float32,
    )
    slot_rows[...] = jnp.where(hits, rank, -1.0)
    slot_columns[...] = slot_rows[...].T
    weight_columns[...] = (
        jnp.where(routes[0:1, :] == named, weights[0:1, :], 0.0)
        + jnp.where(routes[1:2, :] == named, weights[1:2, :], 0.0)
    ).T
    for load in every_load[:6]:
        load.wait()
    lane = lax.broadcasted_iota(jnp.int32, (1, 128), 1)
    first = lane < HEAD_NARROW
    rows_128 = lax.broadcasted_iota(jnp.int32, (128, 128), 0)
    lanes_128 = lax.broadcasted_iota(jnp.int32, (128, 128), 1)
    diagonal = (rows_128 < HEAD_NARROW) == (lanes_128 < HEAD_NARROW)
    flips = []
    for width in (HEAD_WIDE, HEAD_NARROW):
        half_width = width // 2
        upper = lanes_128 % width >= half_width
        origin = jnp.where(upper, lanes_128 - half_width, lanes_128 + half_width)
        flips.append(
            jnp.where(rows_128 == origin, jnp.where(upper, 1.0, -1.0), 0.0).astype(jnp.bfloat16)
        )

    def unit_of(wide_ref, narrow_ref, unit):
        ref = narrow_ref if unit >= 2 else wide_ref
        return ref[:, unit % 2 * 128 : unit % 2 * 128 + 128]

    def per_lane(unit, table):
        if unit < 2:
            return table(unit)
        return jnp.where(first, table(2 * unit - 2), table(2 * unit - 1))

    def heads_of(unit):
        if unit < 2:
            return ((unit, None),)
        return ((2 * unit - 2, first), (2 * unit - 1, ~first))

    def masked(value, keep):
        return value if keep is None else jnp.where(keep, value, jnp.zeros_like(value))

    def swapped(value):
        return pltpu.roll(value, HEAD_NARROW, 1)

    packed = []
    for unit in range(4):
        narrow = unit // 2
        cosine, sine_part = turns[narrow, 0], turns[narrow, 1]
        width = (HEAD_WIDE, HEAD_NARROW)[narrow]
        for n, refs in enumerate(((queries, queries_narrow), (keys, keys_narrow))):
            value = unit_of(*refs, unit)
            flipped = jnp.dot(value, flips[narrow], preferred_element_type=jnp.float32)
            value = value.astype(jnp.float32) * cosine + flipped * sine_part
            if n == 1:
                value = value * width ** (-0.5)
            turned[n, unit] = value.astype(jnp.bfloat16)
        gap = per_lane(
            unit,
            lambda head: log_columns[length - 1 : length, head : head + 1]
            - log_columns[:, head : head + 1],
        )
        weighted = (turned[1, unit].astype(jnp.float32) * jnp.exp(gap)).astype(jnp.bfloat16)
        state = lax.dot_general(
            weighted,
            unit_of(values, values_narrow, unit),
            (((0,), (0,)), ((), ())),
            preferred_element_type=jnp.float32,
        )
        last = log_columns[length - 1 : length, :]
        total_row = per_lane(
            unit, lambda head: jnp.broadcast_to(last[:, head : head + 1], (1, 128))
        )
        if unit == 3:
            state, total_row = swapped(state), swapped(total_row)
        packed.append(state)
        local_total[unit : unit + 1, :] = total_row
    for unit in range(4, 8):
        local_total[unit : unit + 1, :] = jnp.zeros((1, 128), jnp.float32)
    local_state[0] = packed[0].astype(jnp.bfloat16)
    local_state[1] = packed[1].astype(jnp.bfloat16)
    local_state[2] = jnp.where(diagonal, packed[2], packed[3]).astype(jnp.bfloat16)

    def send_state(source, target):
        return remote(
            local_state, states.at[source], s_send.at[target], s_recv.at[source], sp=target
        )

    def send_total(source, target):
        return remote(
            local_total, totals.at[source], t_send.at[target], t_recv.at[source], sp=target
        )

    pl.semaphore_wait(barrier, experts + 1)

    @pl.loop(place + 1, experts)
    def _(target):
        send_state(place, target).start()
        send_total(place, target).start()

    tile = min(length, 256)
    for unit in range(4):
        value = unit_of(values, values_narrow, unit)
        for start in range(0, length, tile):
            stop = start + tile
            steps = lax.broadcasted_iota(jnp.int32, (tile, stop), 0) + start
            causal = steps >= lax.broadcasted_iota(jnp.int32, (tile, stop), 1)
            total = jnp.zeros((tile, 128), jnp.float32)
            for head, keep in heads_of(unit):
                gaps = log_columns[start:stop, head : head + 1] - log_rows[head : head + 1, :stop]
                decay_grid = jnp.exp(jnp.where(causal, gaps, -1e30))
                scores = lax.dot_general(
                    masked(turned[0, unit, start:stop], keep),
                    turned[1, unit, :stop],
                    (((1,), (1,)), ((), ())),
                    preferred_element_type=jnp.float32,
                )
                total += jnp.dot(
                    (scores * decay_grid).astype(jnp.bfloat16),
                    masked(value[:stop], keep),
                    preferred_element_type=jnp.float32,
                )
            inner[unit, start:stop] = total

    def join(source, carried):
        send_state(source, source).wait_recv()
        send_total(source, source).wait_recv()
        fade = jnp.exp(totals[source])
        fade_narrow = jnp.where(diagonal, fade[2:3], fade[3:4])
        return (
            carried[0] * fade[0:1] + states[source, 0].astype(jnp.float32),
            carried[1] * fade[1:2] + states[source, 1].astype(jnp.float32),
            carried[2] * fade_narrow + states[source, 2].astype(jnp.float32),
        )

    nothing = jnp.zeros((128, 128), jnp.float32)
    carried = lax.fori_loop(0, place, join, (nothing, nothing, nothing))
    for unit in range(4):
        state = carried[min(unit, 2)]
        if unit == 2:
            state = jnp.where(diagonal, state, 0.0)
        if unit == 3:
            state = swapped(jnp.where(diagonal, 0.0, state))
        fade = jnp.exp(per_lane(unit, lambda head: log_columns[:, head : head + 1]))
        value = inner[unit] + fade * jnp.dot(
            turned[0, unit], state.astype(jnp.bfloat16), preferred_element_type=jnp.float32
        )

        def mean_of(value):
            if unit < 2:
                return jnp.mean(value, axis=-1, keepdims=True)
            low = jnp.sum(masked(value, first), axis=-1, keepdims=True)
            high = jnp.sum(masked(value, ~first), axis=-1, keepdims=True)
            return jnp.where(first, low, high) / HEAD_NARROW

        value = value - mean_of(value)
        spread = mean_of(value * value)
        mixed[:, unit * 128 : unit * 128 + 128] = (value * lax.rsqrt(spread + norm_eps)).astype(
            jnp.bfloat16
        )

    targets = (across // 2 * 2 + 1 - core, partner, across, mine)
    to_partner = [
        remote(part.at[n], part_in.at[n], a_send.at[n], a_recv.at[n], tp=partner)
        for n in range(2)
    ]
    to_across = remote(cross, cross_in, a_send.at[2], a_recv.at[2], tp=across)
    for load in every_load[6:9]:
        load.wait()
    for n, target in enumerate(targets):
        picked = mixed[pl.ds(pl.multiple_of(target * rows_dev, rows_dev), rows_dev), :]
        part[n] = (
            jnp.dot(picked[:, :256], out_wide[...], preferred_element_type=jnp.float32)
            + jnp.dot(picked[:, 256:], out_narrow[...], preferred_element_type=jnp.float32)
        ).astype(jnp.bfloat16)
        if n < 2:
            to_partner[n].start()
        if n == 2:
            to_partner[0].wait_recv()
            cross[...] = (
                part[2].astype(jnp.float32) + part_in[0].astype(jnp.float32)
            ).astype(jnp.bfloat16)
            to_across.start()
    to_partner[1].wait_recv()
    hidden_state[...] = (
        residual[...].astype(jnp.float32)
        + part[3].astype(jnp.float32)
        + part_in[1].astype(jnp.float32)
    )
    to_across.wait_recv()
    total = hidden_state[...] + cross_in[...].astype(jnp.float32)
    hidden_state[...] = total
    scale_row = lax.rsqrt(jnp.mean(total * total, axis=-1, keepdims=True) + norm_eps)
    normed = (total * scale_row * gain[...]).astype(jnp.bfloat16)

    slot_at = lax.broadcasted_iota(jnp.int32, (capacity, rows_dev), 0).astype(jnp.float32)

    def slots(expert):
        scatter = (slot_rows[pl.ds(expert, 1), :] == slot_at).astype(jnp.bfloat16)
        return jnp.dot(scatter, normed, preferred_element_type=jnp.float32).astype(jnp.bfloat16)

    def dispatch(expert):
        return remote(
            send.at[expert],
            rows.at[place, mine],
            z_send.at[expert],
            z_recv.at[place],
            sp=expert,
        )

    def arrived(source):
        return remote(
            send.at[source], rows.at[source, mine], z_send.at[source], z_recv.at[source], sp=source
        )

    def forward_across(source):
        return remote(
            rows.at[source, mine],
            rows.at[source, mine],
            x_send.at[source],
            x_recv.at[source],
            tp=across,
        )

    def forward_partner(source, n):
        block = (mine, across)[n]
        return remote(
            rows.at[source, block],
            rows.at[source, block],
            p_send.at[source, n],
            p_recv.at[source, n],
            tp=partner,
        )

    def swap(source):
        return remote(
            result.at[source, 1 - core],
            result_in.at[source],
            c_send.at[source],
            c_recv.at[source],
            tp=partner,
        )

    def swap_across(source):
        return remote(
            half.at[source], half_in.at[source], h_send.at[source], h_recv.at[source], tp=across
        )

    def give_back(source):
        return remote(
            summed.at[source],
            returned.at[place],
            r_send.at[source],
            r_recv.at[place],
            sp=source,
        )

    def came_back(expert):
        return remote(
            summed.at[expert],
            returned.at[expert],
            r_send.at[expert],
            r_recv.at[expert],
            sp=expert,
        )

    @pl.loop(1, experts)
    def _(step):
        expert = peer(step)
        send[expert] = slots(expert)
        dispatch(expert).start()

    rows[place, mine] = slots(place)
    forward_across(place).start()
    forward_partner(place, 0).start()

    for load in loads:
        load.wait()

    ff = gate.shape[1]
    ff_step = min(ff, 256)
    out_step = min(model_width, 512)

    def finish_across(source):
        swap_across(source).wait_recv()
        value = (
            result[source, core, side].astype(jnp.float32)
            + result_in[source, side].astype(jnp.float32)
            + half_in[source].astype(jnp.float32)
        ).astype(jnp.bfloat16)

        @pl.when(source == place)
        def _():
            returned[place] = value

        @pl.when(source != place)
        def _():
            summed[source] = value
            give_back(source).start()

    late = min(2, experts - 1)

    def halve(source):
        swap(source).wait_recv()
        half[source] = (
            result[source, core, 1 - side].astype(jnp.float32)
            + result_in[source, 1 - side].astype(jnp.float32)
        ).astype(jnp.bfloat16)
        swap_across(source).start()

    @pl.loop(0, experts)
    def _(step):
        source = peer(step)

        @pl.when(step + 1 < experts)
        def _():
            later = peer(step + 1)
            arrived(later).wait_recv()
            forward_across(later).start()
            forward_partner(later, 0).start()

        forward_across(source).wait_recv()
        forward_partner(source, 1).start()
        forward_partner(source, 0).wait_recv()
        forward_partner(source, 1).wait_recv()
        block = rows[source].reshape(4 * capacity, model_width)
        hidden = []
        for at in range(0, ff, ff_step):
            gate_pre = jnp.dot(
                block, gate[:, at : at + ff_step], preferred_element_type=jnp.float32
            )
            up_pre = jnp.dot(block, up[:, at : at + ff_step], preferred_element_type=jnp.float32)
            hidden.append(activate(gate_pre, up_pre).astype(jnp.bfloat16))
        hidden = jnp.concatenate(hidden, axis=1)
        for at in range(0, model_width, out_step):
            value = jnp.dot(
                hidden, down[:, at : at + out_step], preferred_element_type=jnp.float32
            ).astype(jnp.bfloat16)
            for n in range(4):
                result[source, n % 2, n // 2, :, at : at + out_step] = value[
                    n * capacity : (n + 1) * capacity
                ]
        swap(source).start()

        @pl.when(step >= late)
        def _():
            halve(source)

        @pl.when(step > late)
        def _():
            finish_across(peer(step - 1))

    waiting = experts - 1 if experts > late else None
    for step in range(late - 1, -1, -1):
        halve(peer(step))
        if waiting is not None:
            finish_across(peer(waiting))
        waiting = step
    finish_across(peer(waiting))

    slot_lane = lax.broadcasted_iota(jnp.int32, (rows_dev, capacity), 1).astype(jnp.float32)
    name_lane = lax.broadcasted_iota(jnp.int32, slot_columns.shape, 1)

    def column_of(table, expert):
        kept = jnp.where(name_lane == expert, table[...], 0.0)
        return jnp.sum(kept, axis=1, keepdims=True)

    def add_expert(expert):
        pick = (column_of(slot_columns, expert) == slot_lane).astype(jnp.bfloat16)
        hidden_state[...] += column_of(weight_columns, expert) * jnp.dot(
            pick, returned[expert], preferred_element_type=jnp.float32
        )

    add_expert(place)

    @pl.loop(1, experts)
    def _(step):
        came_back(peer(step)).wait_recv()
        add_expert(peer(step))

    total = hidden_state[...]
    output[...] = total.astype(output.dtype)

    @pl.loop(place + 1, experts)
    def _(target):
        send_state(place, target).wait_send()
        send_total(place, target).wait_send()

    to_partner[0].wait_send()
    to_partner[1].wait_send()
    to_across.wait_send()

    @pl.loop(0, experts)
    def _(step):
        source = peer(step)
        forward_across(source).wait_send()
        forward_partner(source, 0).wait_send()
        forward_partner(source, 1).wait_send()
        swap(source).wait_send()
        swap_across(source).wait_send()

        @pl.when(step >= 1)
        def _():
            dispatch(source).wait_send()
            give_back(source).wait_send()


FINE_ROWS = 32


def rotary_tables(steps):
    grids = []
    for at in (np.arange(0, steps, FINE_ROWS), np.arange(FINE_ROWS)):
        grid = []
        for width in (HEAD_WIDE, HEAD_NARROW):
            half_width = width // 2
            inverse = np.float32(rotary_base) ** (
                -np.arange(half_width, dtype=np.float32) / np.float32(half_width)
            )
            angles = at[:, None] * np.tile(inverse.astype(np.float64), 128 // half_width)
            grid.append(np.stack([np.cos(angles), np.sin(angles)]))
        grids.append(np.stack(grid).astype(np.float32))
    return grids


def layer(mixer_inputs, decays, outs, residual, norm_gain, routes, route_weights, gate, up, down):
    experts = lax.axis_size("sp")
    rows_dev, model_width = residual.shape
    length = mixer_inputs[0].shape[0]
    ff = gate.shape[1]
    limit = max(TOP_K, 3 * rows_dev * TOP_K // (2 * experts))
    capacity = -(-limit // 16) * 16
    named = -(-experts // 8) * 8
    coarse, fine = rotary_tables(experts * length)
    bf16 = jnp.bfloat16
    block = (capacity, model_width)
    dma = pltpu.SemaphoreType.DMA
    vmem = pl.BlockSpec(memory_space=pltpu.VMEM)
    anywhere = pl.BlockSpec(memory_space=pl.ANY)
    return pl.pallas_call(
        functools.partial(tail_kernel, experts, capacity),
        out_shape=jax.ShapeDtypeStruct((rows_dev, model_width), bf16),
        in_specs=[anywhere] * 12 + [vmem] * 7,
        out_specs=vmem,
        scratch_shapes=[
            pltpu.VMEM((6, *mixer_inputs[0].shape), bf16),
            pltpu.VMEM((2, *outs[0].shape), bf16),
            pltpu.VMEM((rows_dev, model_width), bf16),
            pltpu.VMEM((model_width, ff), bf16),
            pltpu.VMEM((model_width, ff), bf16),
            pltpu.VMEM((ff, model_width), bf16),
            pltpu.VMEM((8, length), jnp.float32),
            pltpu.VMEM((8, length), jnp.float32),
            pltpu.VMEM((length, 8), jnp.float32),
            pltpu.VMEM((2, 2, length, 128), jnp.float32),
            pltpu.VMEM((named, rows_dev), jnp.float32),
            pltpu.VMEM((rows_dev, named), jnp.float32),
            pltpu.VMEM((rows_dev, named), jnp.float32),
            pltpu.VMEM((4, rows_dev, model_width), bf16),
            pltpu.VMEM((2, rows_dev, model_width), bf16),
            pltpu.VMEM((rows_dev, model_width), bf16),
            pltpu.VMEM((rows_dev, model_width), bf16),
            pltpu.VMEM((rows_dev, model_width), jnp.float32),
            pltpu.VMEM((experts, *block), bf16),
            pltpu.VMEM((experts, 4, *block), bf16),
            pltpu.VMEM((experts, 2, 2, *block), bf16),
            pltpu.VMEM((experts, 2, *block), bf16),
            pltpu.VMEM((experts, *block), bf16),
            pltpu.VMEM((experts, *block), bf16),
            pltpu.VMEM((experts, *block), bf16),
            pltpu.VMEM((experts, *block), bf16),
            pltpu.VMEM((length, 512), bf16),
            pltpu.VMEM((4, length, 128), jnp.float32),
            pltpu.VMEM((2, 4, length, 128), bf16),
            pltpu.VMEM((3, 128, 128), bf16),
            pltpu.VMEM((8, 128), jnp.float32),
            pltpu.VMEM((experts, 3, 128, 128), bf16),
            pltpu.VMEM((experts, 8, 128), jnp.float32),
            dma((12,)),
            dma((experts,)),
            dma((experts,)),
            dma((experts,)),
            dma((experts,)),
            dma((3,)),
            dma((3,)),
            dma((experts,)),
            dma((experts,)),
            dma((experts,)),
            dma((experts,)),
            dma((experts, 2)),
            dma((experts, 2)),
            dma((experts,)),
            dma((experts,)),
            dma((experts,)),
            dma((experts,)),
            dma((experts,)),
            dma((experts,)),
        ],
        compiler_params=pltpu.CompilerParams(
            collective_id=1, has_side_effects=True, vmem_limit_bytes=60 * 1024 * 1024
        ),
    )(
        *mixer_inputs,
        *outs,
        residual,
        gate,
        up,
        down,
        *decays,
        coarse,
        fine,
        norm_gain.reshape(1, model_width),
        routes.T,
        route_weights.T,
    )


def body(
    query_wide,
    key_wide,
    value_wide,
    decay_wide,
    query_narrow,
    key_narrow,
    value_narrow,
    decay_narrow,
    residual,
    out_wide,
    out_narrow,
    norm_gain,
    routes,
    route_weights,
    expert_gate,
    expert_up,
    expert_down,
):
    return layer(
        (
            query_wide,
            query_narrow,
            key_wide,
            key_narrow,
            value_wide,
            value_narrow,
        ),
        (decay_wide.T, decay_narrow.T),
        (out_wide, out_narrow),
        residual,
        norm_gain,
        routes,
        route_weights,
        expert_gate[0],
        expert_up[0],
        expert_down[0],
    )


def solution(mesh):
    placed = (
        P(("grp", "sp"), "tp"),
        P(("grp", "sp"), "tp"),
        P(("grp", "sp"), "tp"),
        P(("grp", "sp"), "tp"),
        P(("grp", "sp"), "tp"),
        P(("grp", "sp"), "tp"),
        P(("grp", "sp"), "tp"),
        P(("grp", "sp"), "tp"),
        P(("grp", "sp", "tp"), None),
        P("tp", None),
        P("tp", None),
        P(),
        P(("grp", "sp", "tp"), None),
        P(("grp", "sp", "tp"), None),
        P("sp", None, "tp"),
        P("sp", None, "tp"),
        P("sp", "tp", None),
    )
    return jax.shard_map(
        body, mesh=mesh, in_specs=placed, out_specs=P(("grp", "sp", "tp"), None), check_vma=False
    )
```

```python
import functools

import jax
import jax.numpy as jnp
import numpy as np
from jax import lax
from jax.experimental import pallas as pl
from jax.experimental.pallas import tpu as pltpu
from jax.sharding import PartitionSpec as P

HEAD_WIDE = 128
HEAD_NARROW = 64
TOP_K = 2


norm_eps = 1e-05
clamp_limit = 7.0
swish_alpha = 1.702
rotary_base = 10000.0


def activate(gate_pre, up_pre):
    gate_clip = jnp.minimum(gate_pre, clamp_limit)
    up_clip = jnp.clip(up_pre, -clamp_limit, clamp_limit)
    return gate_clip * jax.nn.sigmoid(swish_alpha * gate_clip) * (up_clip + 1.0)


MESH = pl.DeviceIdType.MESH


def tail_kernel(
    experts,
    capacity,
    queries_hbm,
    queries_narrow_hbm,
    keys_hbm,
    keys_narrow_hbm,
    values_hbm,
    values_narrow_hbm,
    out_wide_hbm,
    out_narrow_hbm,
    residual_hbm,
    gate_hbm,
    up_hbm,
    down_hbm,
    decay_wide,
    decay_narrow,
    coarse,
    fine,
    gain,
    routes,
    weights,
    output,
    mixer_in,
    outs_in,
    residual,
    gate,
    up,
    down,
    decays,
    log_rows,
    log_columns,
    turns,
    slot_rows,
    slot_columns,
    weight_columns,
    part,
    part_in,
    cross,
    cross_in,
    hidden_state,
    send,
    rows,
    hidden_own,
    hidden_in,
    result,
    returned,
    mixed,
    inner,
    turned,
    local_state,
    local_total,
    states,
    totals,
    load_sem,
    s_send,
    s_recv,
    t_send,
    t_recv,
    a_send,
    a_recv,
    z_send,
    z_recv,
    x_send,
    x_recv,
    p_send,
    p_recv,
    h_send,
    h_recv,
    r_send,
    r_recv,
    w_send,
    w_recv,
    y_send,
    y_recv,
    d_send,
    d_recv,
):
    place = lax.axis_index("sp")
    mine = lax.axis_index("tp")
    core, side = mine % 2, mine // 2
    partner = side * 2 + (1 - core)
    across = (1 - side) * 2 + core
    diagonal_peer = (1 - side) * 2 + 1 - core
    group = lax.axis_index("grp")
    model_width = residual.shape[1]
    half_model = model_width // 2

    def remote(src, dst, send_sem, recv_sem, **where):
        return pltpu.make_async_remote_copy(
            src_ref=src,
            dst_ref=dst,
            send_sem=send_sem,
            recv_sem=recv_sem,
            device_id=where,
            device_id_type=MESH,
        )

    order = (0, 2, 3, 1)
    short = experts == len(order)

    def peer(step):
        if short and isinstance(step, int):
            return place ^ order[step]
        return lax.rem(place + step, experts) if experts & (experts - 1) else place ^ step

    def half_of(which):
        return pl.ds(pl.multiple_of(which * half_model, half_model), half_model)

    ff = gate.shape[1]
    pieces = 8
    piece_rows = ff // pieces
    far_core = (core + group) % 2
    far = (1 - side) * 2 + far_core

    def piece_at(n):
        return pl.ds(n * piece_rows, piece_rows)

    def down_far(n):
        return remote(
            down_hbm.at[piece_at(n), half_of(far_core)],
            down.at[2 + group, piece_at(n)],
            w_send.at[n],
            w_recv.at[n],
            tp=far,
        )

    def down_group(n, slot):
        return remote(
            down.at[slot, piece_at(n)],
            down.at[slot, piece_at(n)],
            y_send.at[n],
            y_recv.at[n],
            grp=1 - group,
        )

    def pass_down(n):
        down_far(n).wait_recv()
        down_group(n, 2 + group).start()

    down_partner = remote(
        down_hbm.at[:, half_of(1 - core)], down.at[1], d_send.at[0], d_recv.at[0], tp=partner
    )

    sources = (
        (keys_hbm, mixer_in.at[2]),
        (keys_narrow_hbm, mixer_in.at[3]),
        (values_hbm, mixer_in.at[4]),
        (values_narrow_hbm, mixer_in.at[5]),
        (queries_hbm, mixer_in.at[0]),
        (queries_narrow_hbm, mixer_in.at[1]),
        (out_wide_hbm, outs_in.at[0]),
        (out_narrow_hbm, outs_in.at[1]),
        (residual_hbm, residual),
        (gate_hbm, gate),
        (up_hbm, up),
        (down_hbm.at[:, half_of(core)], down.at[0]),
    )
    every_load = [
        pltpu.make_async_copy(src, dst, load_sem.at[n]) for n, (src, dst) in enumerate(sources)
    ]
    for load in every_load:
        load.start()
    loads = every_load[9:]
    queries, queries_narrow = mixer_in.at[0], mixer_in.at[1]
    keys, keys_narrow = mixer_in.at[2], mixer_in.at[3]
    values, values_narrow = mixer_in.at[4], mixer_in.at[5]
    out_wide, out_narrow = outs_in.at[0], outs_in.at[1]

    barrier = pltpu.get_barrier_semaphore()
    for target in (partner, across, diagonal_peer):
        pl.semaphore_signal(barrier, inc=1, device_id={"tp": target}, device_id_type=MESH)
    pl.semaphore_signal(barrier, inc=1, device_id={"grp": 1 - group}, device_id_type=MESH)

    @pl.loop(1, experts)
    def _(step):
        pl.semaphore_signal(barrier, inc=1, device_id={"sp": peer(step)}, device_id_type=MESH)
        pl.semaphore_signal(
            barrier, inc=1, device_id={"sp": peer(step), "tp": partner}, device_id_type=MESH
        )

    length = queries.shape[0]
    rows_dev = residual.shape[0]
    fine_rows = fine.shape[2]
    coarse_rows = length // fine_rows
    at_coarse = pl.multiple_of(place * coarse_rows, coarse_rows)
    for narrow in range(2):
        cosine_fine, sine_fine = fine[narrow, 0], fine[narrow, 1]
        cosine_coarse = coarse[narrow, 0, pl.ds(at_coarse, coarse_rows), :]
        sine_coarse = coarse[narrow, 1, pl.ds(at_coarse, coarse_rows), :]
        for at in range(coarse_rows):
            cosine, sine_part = cosine_coarse[at : at + 1], sine_coarse[at : at + 1]
            span = slice(at * fine_rows, (at + 1) * fine_rows)
            turns[narrow, 0, span] = cosine * cosine_fine - sine_part * sine_fine
            turns[narrow, 1, span] = sine_part * cosine_fine + cosine * sine_fine

    pl.semaphore_wait(barrier, 2 * experts + 2)
    early = pieces - 4
    for n in range(early):
        down_far(n).start()
    down_partner.start()

    def pieces_of(value):
        high = value.astype(jnp.bfloat16)
        rest = value - high.astype(jnp.float32)
        middle = rest.astype(jnp.bfloat16)
        low = (rest - middle.astype(jnp.float32)).astype(jnp.bfloat16)
        return high, middle, low

    row_at = lax.broadcasted_iota(jnp.int32, (128, 128), 0)
    lane_at = lax.broadcasted_iota(jnp.int32, (128, 128), 1)
    up_to = (row_at <= lane_at).astype(jnp.bfloat16)
    heads_wide, heads_narrow = decay_wide.shape[0], decay_narrow.shape[0]
    decays[...] = jnp.zeros_like(decays)
    decays[0:heads_wide, :] = decay_wide[...]
    decays[heads_wide : heads_wide + heads_narrow, :] = decay_narrow[...]
    running = jnp.zeros((8, 1), jnp.float32)
    for at in range(0, length, 128):
        within = running
        for piece in pieces_of(decays[:, at : at + 128]):
            within = within + jnp.dot(piece, up_to, preferred_element_type=jnp.float32)
        log_rows[:, at : at + 128] = within
        log_columns[at : at + 128, :] = within.T
        running = within[:, 127:128]

    for load in every_load[:4]:
        load.wait()
    lane = lax.broadcasted_iota(jnp.int32, (1, 128), 1)
    first = lane < HEAD_NARROW
    rows_128 = lax.broadcasted_iota(jnp.int32, (128, 128), 0)
    lanes_128 = lax.broadcasted_iota(jnp.int32, (128, 128), 1)
    diagonal = (rows_128 < HEAD_NARROW) == (lanes_128 < HEAD_NARROW)
    flips = []
    for width in (HEAD_WIDE, HEAD_NARROW):
        half_width = width // 2
        upper = lanes_128 % width >= half_width
        origin = jnp.where(upper, lanes_128 - half_width, lanes_128 + half_width)
        flips.append(
            jnp.where(rows_128 == origin, jnp.where(upper, 1.0, -1.0), 0.0).astype(jnp.bfloat16)
        )

    def unit_of(wide_ref, narrow_ref, unit):
        ref = narrow_ref if unit >= 2 else wide_ref
        return ref[:, unit % 2 * 128 : unit % 2 * 128 + 128]

    def per_lane(unit, table):
        if unit < 2:
            return table(unit)
        return jnp.where(first, table(2 * unit - 2), table(2 * unit - 1))

    def heads_of(unit):
        if unit < 2:
            return ((unit, None),)
        return ((2 * unit - 2, first), (2 * unit - 1, ~first))

    def masked(value, keep):
        return value if keep is None else jnp.where(keep, value, jnp.zeros_like(value))

    def swapped(value):
        return pltpu.roll(value, HEAD_NARROW, 1)

    def rotated(refs, unit):
        narrow = unit // 2
        value = unit_of(*refs, unit)
        flipped = jnp.dot(value, flips[narrow], preferred_element_type=jnp.float32)
        return value.astype(jnp.float32) * turns[narrow, 0] + flipped * turns[narrow, 1]

    packed = []
    for unit in range(4):
        narrow = unit // 2
        width = (HEAD_WIDE, HEAD_NARROW)[narrow]
        value = rotated((keys, keys_narrow), unit)
        turned[1, unit] = (value * width ** (-0.5)).astype(jnp.bfloat16)
        gap = per_lane(
            unit,
            lambda head: log_columns[length - 1 : length, head : head + 1]
            - log_columns[:, head : head + 1],
        )
        weighted = (turned[1, unit].astype(jnp.float32) * jnp.exp(gap)).astype(jnp.bfloat16)
        state = lax.dot_general(
            weighted,
            unit_of(values, values_narrow, unit),
            (((0,), (0,)), ((), ())),
            preferred_element_type=jnp.float32,
        )
        last = log_columns[length - 1 : length, :]
        total_row = per_lane(
            unit, lambda head: jnp.broadcast_to(last[:, head : head + 1], (1, 128))
        )
        if unit == 3:
            state, total_row = swapped(state), swapped(total_row)
        packed.append(state)
        local_total[unit : unit + 1, :] = total_row
    for unit in range(4, 8):
        local_total[unit : unit + 1, :] = jnp.zeros((1, 128), jnp.float32)
    local_state[0] = packed[0].astype(jnp.bfloat16)
    local_state[1] = packed[1].astype(jnp.bfloat16)
    local_state[2] = jnp.where(diagonal, packed[2], packed[3]).astype(jnp.bfloat16)

    def send_state(source, target):
        return remote(
            local_state, states.at[source], s_send.at[target], s_recv.at[source], sp=target
        )

    def send_total(source, target):
        return remote(
            local_total, totals.at[source], t_send.at[target], t_recv.at[source], sp=target
        )

    @pl.loop(place + 1, experts)
    def _(target):
        send_state(place, target).start()
        send_total(place, target).start()

    named = lax.broadcasted_iota(jnp.int32, (slot_rows.shape[0], rows_dev), 0)
    hits = (routes[0:1, :] == named) | (routes[1:2, :] == named)
    earlier = lax.broadcasted_iota(jnp.int32, (rows_dev, rows_dev), 0) < lax.broadcasted_iota(
        jnp.int32, (rows_dev, rows_dev), 1
    )
    rank = jnp.dot(
        hits.astype(jnp.bfloat16),
        earlier.astype(jnp.bfloat16),
        preferred_element_type=jnp.float32,
    )
    slot_rows[...] = jnp.where(hits, rank, -1.0)
    slot_columns[...] = slot_rows[...].T
    weight_columns[...] = (
        jnp.where(routes[0:1, :] == named, weights[0:1, :], 0.0)
        + jnp.where(routes[1:2, :] == named, weights[1:2, :], 0.0)
    ).T
    for load in every_load[4:6]:
        load.wait()
    for unit in range(4):
        turned[0, unit] = rotated((queries, queries_narrow), unit).astype(jnp.bfloat16)

    tile = min(length, 256)
    for unit in range(4):
        value = unit_of(values, values_narrow, unit)
        for start in range(0, length, tile):
            stop = start + tile
            steps = lax.broadcasted_iota(jnp.int32, (tile, stop), 0) + start
            causal = steps >= lax.broadcasted_iota(jnp.int32, (tile, stop), 1)
            total = jnp.zeros((tile, 128), jnp.float32)
            for head, keep in heads_of(unit):
                gaps = log_columns[start:stop, head : head + 1] - log_rows[head : head + 1, :stop]
                decay_grid = jnp.exp(jnp.where(causal, gaps, -1e30))
                scores = lax.dot_general(
                    masked(turned[0, unit, start:stop], keep),
                    turned[1, unit, :stop],
                    (((1,), (1,)), ((), ())),
                    preferred_element_type=jnp.float32,
                )
                total += jnp.dot(
                    (scores * decay_grid).astype(jnp.bfloat16),
                    masked(value[:stop], keep),
                    preferred_element_type=jnp.float32,
                )
            inner[unit, start:stop] = total

    def join(source, carried):
        send_state(source, source).wait_recv()
        send_total(source, source).wait_recv()
        fade = jnp.exp(totals[source])
        fade_narrow = jnp.where(diagonal, fade[2:3], fade[3:4])
        return (
            carried[0] * fade[0:1] + states[source, 0].astype(jnp.float32),
            carried[1] * fade[1:2] + states[source, 1].astype(jnp.float32),
            carried[2] * fade_narrow + states[source, 2].astype(jnp.float32),
        )

    pass_down(0)
    nothing = jnp.zeros((128, 128), jnp.float32)
    carried = lax.fori_loop(0, place, join, (nothing, nothing, nothing))
    for unit in range(4):
        state = carried[min(unit, 2)]
        if unit == 2:
            state = jnp.where(diagonal, state, 0.0)
        if unit == 3:
            state = swapped(jnp.where(diagonal, 0.0, state))
        fade = jnp.exp(per_lane(unit, lambda head: log_columns[:, head : head + 1]))
        value = inner[unit] + fade * jnp.dot(
            turned[0, unit], state.astype(jnp.bfloat16), preferred_element_type=jnp.float32
        )

        def mean_of(value):
            if unit < 2:
                return jnp.mean(value, axis=-1, keepdims=True)
            low = jnp.sum(masked(value, first), axis=-1, keepdims=True)
            high = jnp.sum(masked(value, ~first), axis=-1, keepdims=True)
            return jnp.where(first, low, high) / HEAD_NARROW

        value = value - mean_of(value)
        spread = mean_of(value * value)
        mixed[:, unit * 128 : unit * 128 + 128] = (value * lax.rsqrt(spread + norm_eps)).astype(
            jnp.bfloat16
        )

    columns = 4
    width = model_width // columns

    def to_partner(n, at):
        where = (n, slice(None), pl.ds(at * width, width))
        return remote(
            part.at[where], part_in.at[where], a_send.at[n, at], a_recv.at[n, at], tp=partner
        )

    def to_across(at):
        where = (slice(None), pl.ds(at * width, width))
        return remote(
            cross.at[where], cross_in.at[where], a_send.at[2, at], a_recv.at[2, at], tp=across
        )

    for load in every_load[6:9]:
        load.wait()

    def projected(target, at):
        picked = mixed[pl.ds(pl.multiple_of(target * rows_dev, rows_dev), rows_dev), :]
        span = slice(at * width, (at + 1) * width)
        return jnp.dot(
            picked[:, :256], out_wide[:, span], preferred_element_type=jnp.float32
        ) + jnp.dot(picked[:, 256:], out_narrow[:, span], preferred_element_type=jnp.float32)

    for at in range(columns):
        span = slice(at * width, (at + 1) * width)
        part[0, :, span] = projected(diagonal_peer, at).astype(jnp.bfloat16)
        to_partner(0, at).start()
    for at in range(columns):
        span = slice(at * width, (at + 1) * width)
        value = projected(across, at)
        to_partner(0, at).wait_recv()
        cross[:, span] = (value + part_in[0, :, span].astype(jnp.float32)).astype(jnp.bfloat16)
        to_across(at).start()
    pass_down(1)
    for at in range(columns):
        span = slice(at * width, (at + 1) * width)
        part[1, :, span] = projected(partner, at).astype(jnp.bfloat16)
        to_partner(1, at).start()
    for at in range(columns):
        span = slice(at * width, (at + 1) * width)
        value = residual[:, span].astype(jnp.float32) + projected(mine, at)
        to_partner(1, at).wait_recv()
        hidden_state[:, span] = value + part_in[1, :, span].astype(jnp.float32)
    for n in range(2, early):
        pass_down(n)
    for at in range(columns):
        to_across(at).wait_recv()
    total = hidden_state[...] + cross_in[...].astype(jnp.float32)
    hidden_state[...] = total
    scale_row = lax.rsqrt(jnp.mean(total * total, axis=-1, keepdims=True) + norm_eps)
    normed = (total * scale_row * gain[...]).astype(jnp.bfloat16)

    slot_at = lax.broadcasted_iota(jnp.int32, (capacity, rows_dev), 0).astype(jnp.float32)

    def slots(expert):
        scatter = (slot_rows[pl.ds(expert, 1), :] == slot_at).astype(jnp.bfloat16)
        return jnp.dot(scatter, normed, preferred_element_type=jnp.float32).astype(jnp.bfloat16)

    def dispatch(expert):
        return remote(
            send.at[expert],
            rows.at[place, mine],
            z_send.at[expert],
            z_recv.at[place],
            sp=expert,
        )

    def arrived(source):
        return remote(
            send.at[source], rows.at[source, mine], z_send.at[source], z_recv.at[source], sp=source
        )

    def forward_across(source):
        return remote(
            rows.at[source, mine],
            rows.at[source, mine],
            x_send.at[source],
            x_recv.at[source],
            tp=across,
        )

    def forward_partner(source, n):
        block = (mine, across)[n]
        return remote(
            rows.at[source, block],
            rows.at[source, block],
            p_send.at[source, n],
            p_recv.at[source, n],
            tp=partner,
        )

    def hidden_across(source):
        return remote(
            hidden_own.at[source, 1 - side],
            hidden_in.at[source, 1],
            h_send.at[source, 1],
            h_recv.at[source, 1],
            tp=across,
        )

    def hidden_partner(source):
        return remote(
            hidden_own.at[source, side],
            hidden_in.at[source, 0],
            h_send.at[source, 0],
            h_recv.at[source, 0],
            tp=partner,
        )

    def hidden_forward(source):
        return remote(
            hidden_in.at[source, 1],
            hidden_in.at[source, 2],
            h_send.at[source, 2],
            h_recv.at[source, 2],
            tp=partner,
        )

    def give_back(source):
        return remote(
            result.at[source, core],
            returned.at[place, core],
            r_send.at[source, 0],
            r_recv.at[place, core],
            sp=source,
        )

    def give_partner(source):
        return remote(
            result.at[source, 1 - core],
            returned.at[place, core],
            r_send.at[source, 1],
            r_recv.at[place, core],
            sp=source,
            tp=partner,
        )

    def came_back(expert, which):
        return remote(
            result.at[expert, 0],
            returned.at[expert, which],
            r_send.at[expert, 0],
            r_recv.at[expert, which],
            sp=expert,
        )

    @pl.loop(1, experts)
    def _(step):
        expert = peer(step)
        send[expert] = slots(expert)
        dispatch(expert).start()

    rows[place, mine] = slots(place)

    for load in loads:
        load.wait()

    ff_step = min(ff, 256)
    out_step = min(half_model, 512)

    def spread(source):
        hidden_across(source).wait_recv()
        hidden_forward(source).start()

    def finish(source):
        hidden_partner(source).wait_recv()
        hidden_forward(source).wait_recv()
        for at in range(0, half_model, out_step):
            span = slice(at, at + out_step)
            value = jnp.dot(
                hidden_own[source, side], down[0, :, span], preferred_element_type=jnp.float32
            )
            for n in range(3):
                value = value + jnp.dot(
                    hidden_in[source, n], down[n + 1, :, span], preferred_element_type=jnp.float32
                )
            value = value.astype(jnp.bfloat16)
            for n in range(2):
                result[source, n, :, span] = value[n * capacity : (n + 1) * capacity]

        @pl.when(source == place)
        def _():
            returned[place, core] = result[place, core]
            remote(
                result.at[place, 1 - core],
                returned.at[place, core],
                r_send.at[place, 1],
                r_recv.at[place, core],
                tp=partner,
            ).start()

        @pl.when(source != place)
        def _():
            give_back(source).start()
            give_partner(source).start()

    def take(step):
        later = peer(step)
        arrived(later).wait_recv()
        forward_across(later).start()
        forward_partner(later, 0).start()

    def expand(source):
        forward_across(source).wait_recv()
        forward_partner(source, 1).start()
        forward_partner(source, 0).wait_recv()
        forward_partner(source, 1).wait_recv()
        block = rows[source].reshape(4 * capacity, model_width)
        for at in range(0, ff, ff_step):
            span = slice(at, at + ff_step)
            gate_pre = jnp.dot(block, gate[:, span], preferred_element_type=jnp.float32)
            up_pre = jnp.dot(block, up[:, span], preferred_element_type=jnp.float32)
            value = activate(gate_pre, up_pre).astype(jnp.bfloat16)
            for n in range(2):
                hidden_own[source, n, :, span] = value[2 * n * capacity : 2 * (n + 1) * capacity]

    def swap_hidden(source):
        hidden_across(source).start()
        hidden_partner(source).start()

    if short:
        for n in range(early, pieces):
            down_far(n).start()
        forward_across(place).start()
        forward_partner(place, 0).start()
        take(1)
        expand(place)
        take(3)
        for n in range(early, pieces):
            pass_down(n)
        expand(peer(1))
        swap_hidden(peer(1))
        take(2)
        expand(peer(3))
        swap_hidden(peer(3))
        down_partner.wait_recv()
        for n in range(pieces):
            down_group(n, 3 - group).wait_recv()
        spread(peer(1))
        finish(peer(1))
        expand(peer(2))
        swap_hidden(peer(2))
        spread(peer(3))
        finish(peer(3))
        spread(peer(2))
        finish(peer(2))
        swap_hidden(place)
        spread(place)
        finish(place)
    else:
        forward_across(place).start()
        forward_partner(place, 0).start()
        take(1)
        for n in range(early, pieces):
            down_far(n).start()
        expand(place)

        @pl.loop(1, experts)
        def _(step):
            source = peer(step)
            expand(source)
            swap_hidden(source)

            @pl.when(step == 1)
            def _():
                for n in range(early, pieces):
                    pass_down(n)

            @pl.when(step + 1 < experts)
            def _():
                take(step + 1)

            @pl.when(step + 1 == experts)
            def _():
                swap_hidden(place)

            @pl.when(step == 1)
            def _():
                down_partner.wait_recv()
                for n in range(pieces):
                    down_group(n, 3 - group).wait_recv()

            spread(source)
            finish(source)

        spread(place)
        finish(place)

    slot_lane = lax.broadcasted_iota(jnp.int32, (rows_dev, capacity), 1).astype(jnp.float32)
    name_lane = lax.broadcasted_iota(jnp.int32, slot_columns.shape, 1)

    def column_of(table, expert):
        kept = jnp.where(name_lane == expert, table[...], 0.0)
        return jnp.sum(kept, axis=1, keepdims=True)

    def add_expert(expert):
        pick = (column_of(slot_columns, expert) == slot_lane).astype(jnp.bfloat16)
        weight = column_of(weight_columns, expert)
        for n in range(2):
            span = slice(n * half_model, (n + 1) * half_model)
            hidden_state[:, span] += weight * jnp.dot(
                pick, returned[expert, n], preferred_element_type=jnp.float32
            )

    came_back(place, 1 - core).wait_recv()
    add_expert(place)

    @pl.loop(1, experts)
    def _(step):
        expert = peer(step)
        came_back(expert, 0).wait_recv()
        came_back(expert, 1).wait_recv()
        add_expert(expert)

    total = hidden_state[...]
    output[...] = total.astype(output.dtype)

    @pl.loop(place + 1, experts)
    def _(target):
        send_state(place, target).wait_send()
        send_total(place, target).wait_send()

    for at in range(columns):
        to_partner(0, at).wait_send()
        to_partner(1, at).wait_send()
        to_across(at).wait_send()
    for n in range(pieces):
        down_far(n).wait_send()
        down_group(n, 2 + group).wait_send()
    down_partner.wait_send()

    @pl.loop(0, experts)
    def _(step):
        source = peer(step)
        forward_across(source).wait_send()
        forward_partner(source, 0).wait_send()
        forward_partner(source, 1).wait_send()
        hidden_across(source).wait_send()
        hidden_partner(source).wait_send()
        hidden_forward(source).wait_send()
        give_partner(source).wait_send()

        @pl.when(step >= 1)
        def _():
            dispatch(source).wait_send()
            give_back(source).wait_send()


FINE_ROWS = 32


def rotary_tables(steps):
    grids = []
    for at in (np.arange(0, steps, FINE_ROWS), np.arange(FINE_ROWS)):
        grid = []
        for width in (HEAD_WIDE, HEAD_NARROW):
            half_width = width // 2
            inverse = np.float32(rotary_base) ** (
                -np.arange(half_width, dtype=np.float32) / np.float32(half_width)
            )
            angles = at[:, None] * np.tile(inverse.astype(np.float64), 128 // half_width)
            grid.append(np.stack([np.cos(angles), np.sin(angles)]))
        grids.append(np.stack(grid).astype(np.float32))
    return grids


def layer(mixer_inputs, decays, outs, residual, norm_gain, routes, route_weights, gate, up, down):
    experts = lax.axis_size("sp")
    rows_dev, model_width = residual.shape
    length = mixer_inputs[0].shape[0]
    ff = gate.shape[1]
    limit = max(TOP_K, 3 * rows_dev * TOP_K // (2 * experts))
    capacity = -(-limit // 16) * 16
    named = -(-experts // 8) * 8
    coarse, fine = rotary_tables(experts * length)
    bf16 = jnp.bfloat16
    block = (capacity, model_width)
    dma = pltpu.SemaphoreType.DMA
    vmem = pl.BlockSpec(memory_space=pltpu.VMEM)
    anywhere = pl.BlockSpec(memory_space=pl.ANY)
    return pl.pallas_call(
        functools.partial(tail_kernel, experts, capacity),
        out_shape=jax.ShapeDtypeStruct((rows_dev, model_width), bf16),
        in_specs=[anywhere] * 12 + [vmem] * 7,
        out_specs=vmem,
        scratch_shapes=[
            pltpu.VMEM((6, *mixer_inputs[0].shape), bf16),
            pltpu.VMEM((2, *outs[0].shape), bf16),
            pltpu.VMEM((rows_dev, model_width), bf16),
            pltpu.VMEM((model_width, ff), bf16),
            pltpu.VMEM((model_width, ff), bf16),
            pltpu.VMEM((4, ff, model_width // 2), bf16),
            pltpu.VMEM((8, length), jnp.float32),
            pltpu.VMEM((8, length), jnp.float32),
            pltpu.VMEM((length, 8), jnp.float32),
            pltpu.VMEM((2, 2, length, 128), jnp.float32),
            pltpu.VMEM((named, rows_dev), jnp.float32),
            pltpu.VMEM((rows_dev, named), jnp.float32),
            pltpu.VMEM((rows_dev, named), jnp.float32),
            pltpu.VMEM((4, rows_dev, model_width), bf16),
            pltpu.VMEM((2, rows_dev, model_width), bf16),
            pltpu.VMEM((rows_dev, model_width), bf16),
            pltpu.VMEM((rows_dev, model_width), bf16),
            pltpu.VMEM((rows_dev, model_width), jnp.float32),
            pltpu.VMEM((experts, *block), bf16),
            pltpu.VMEM((experts, 4, *block), bf16),
            pltpu.VMEM((experts, 2, 2 * capacity, ff), bf16),
            pltpu.VMEM((experts, 3, 2 * capacity, ff), bf16),
            pltpu.VMEM((experts, 2, capacity, model_width // 2), bf16),
            pltpu.VMEM((experts, 2, capacity, model_width // 2), bf16),
            pltpu.VMEM((length, 512), bf16),
            pltpu.VMEM((4, length, 128), jnp.float32),
            pltpu.VMEM((2, 4, length, 128), bf16),
            pltpu.VMEM((3, 128, 128), bf16),
            pltpu.VMEM((8, 128), jnp.float32),
            pltpu.VMEM((experts, 3, 128, 128), bf16),
            pltpu.VMEM((experts, 8, 128), jnp.float32),
            dma((12,)),
            dma((experts,)),
            dma((experts,)),
            dma((experts,)),
            dma((experts,)),
            dma((3, 4)),
            dma((3, 4)),
            dma((experts,)),
            dma((experts,)),
            dma((experts,)),
            dma((experts,)),
            dma((experts, 2)),
            dma((experts, 2)),
            dma((experts, 3)),
            dma((experts, 3)),
            dma((experts, 2)),
            dma((experts, 2)),
            dma((8,)),
            dma((8,)),
            dma((8,)),
            dma((8,)),
            dma((1,)),
            dma((1,)),
        ],
        compiler_params=pltpu.CompilerParams(
            collective_id=1, has_side_effects=True, vmem_limit_bytes=60 * 1024 * 1024
        ),
    )(
        *mixer_inputs,
        *outs,
        residual,
        gate,
        up,
        down,
        *decays,
        coarse,
        fine,
        norm_gain.reshape(1, model_width),
        routes.T,
        route_weights.T,
    )


def body(
    query_wide,
    key_wide,
    value_wide,
    decay_wide,
    query_narrow,
    key_narrow,
    value_narrow,
    decay_narrow,
    residual,
    out_wide,
    out_narrow,
    norm_gain,
    routes,
    route_weights,
    expert_gate,
    expert_up,
    expert_down,
):
    return layer(
        (
            query_wide,
            query_narrow,
            key_wide,
            key_narrow,
            value_wide,
            value_narrow,
        ),
        (decay_wide.T, decay_narrow.T),
        (out_wide, out_narrow),
        residual,
        norm_gain,
        routes,
        route_weights,
        expert_gate[0],
        expert_up[0],
        expert_down[0],
    )


def solution(mesh):
    placed = (
        P(("grp", "sp"), "tp"),
        P(("grp", "sp"), "tp"),
        P(("grp", "sp"), "tp"),
        P(("grp", "sp"), "tp"),
        P(("grp", "sp"), "tp"),
        P(("grp", "sp"), "tp"),
        P(("grp", "sp"), "tp"),
        P(("grp", "sp"), "tp"),
        P(("grp", "sp", "tp"), None),
        P("tp", None),
        P("tp", None),
        P(),
        P(("grp", "sp", "tp"), None),
        P(("grp", "sp", "tp"), None),
        P("sp", None, "tp"),
        P("sp", None, "tp"),
        P("sp", "tp", None),
    )
    return jax.shard_map(
        body, mesh=mesh, in_specs=placed, out_specs=P(("grp", "sp", "tp"), None), check_vma=False
    )
```

```python
import functools

import jax
import jax.numpy as jnp
import numpy as np
from jax import lax
from jax.experimental import pallas as pl
from jax.experimental.pallas import tpu as pltpu
from jax.sharding import PartitionSpec as P

HEAD_WIDE = 128
HEAD_NARROW = 64
TOP_K = 2


norm_eps = 1e-05
clamp_limit = 7.0
swish_alpha = 1.702
rotary_base = 10000.0


def activate(gate_pre, up_pre):
    gate_clip = jnp.minimum(gate_pre, clamp_limit)
    up_clip = jnp.clip(up_pre, -clamp_limit, clamp_limit)
    return gate_clip * jax.nn.sigmoid(swish_alpha * gate_clip) * (up_clip + 1.0)


MESH = pl.DeviceIdType.MESH


def tail_kernel(
    experts,
    capacity,
    queries_hbm,
    queries_narrow_hbm,
    keys_hbm,
    keys_narrow_hbm,
    values_hbm,
    values_narrow_hbm,
    out_wide_hbm,
    out_narrow_hbm,
    residual_hbm,
    gate_hbm,
    up_hbm,
    down_hbm,
    decay_wide,
    decay_narrow,
    coarse,
    fine,
    gain,
    routes,
    weights,
    output,
    mixer_in,
    outs_in,
    residual,
    gate,
    up,
    down,
    decays,
    log_rows,
    log_columns,
    turns,
    slot_rows,
    slot_columns,
    weight_columns,
    part,
    part_in,
    cross,
    cross_in,
    hidden_state,
    send,
    rows,
    hidden_own,
    hidden_in,
    result,
    returned,
    mixed,
    inner,
    turned,
    local_state,
    local_total,
    states,
    totals,
    load_sem,
    s_send,
    s_recv,
    t_send,
    t_recv,
    a_send,
    a_recv,
    z_send,
    z_recv,
    x_send,
    x_recv,
    p_send,
    p_recv,
    h_send,
    h_recv,
    r_send,
    r_recv,
    w_send,
    w_recv,
    y_send,
    y_recv,
    d_send,
    d_recv,
):
    place = lax.axis_index("sp")
    mine = lax.axis_index("tp")
    core, side = mine % 2, mine // 2
    partner = side * 2 + (1 - core)
    across = (1 - side) * 2 + core
    diagonal_peer = (1 - side) * 2 + 1 - core
    group = lax.axis_index("grp")
    model_width = residual.shape[1]
    half_model = model_width // 2

    def remote(src, dst, send_sem, recv_sem, **where):
        return pltpu.make_async_remote_copy(
            src_ref=src,
            dst_ref=dst,
            send_sem=send_sem,
            recv_sem=recv_sem,
            device_id=where,
            device_id_type=MESH,
        )

    order = (0, 1, 2, 3)
    short = experts == len(order)

    def peer(step):
        if short and isinstance(step, int):
            return place ^ order[step]
        return lax.rem(place + step, experts) if experts & (experts - 1) else place ^ step

    def half_of(which):
        return pl.ds(pl.multiple_of(which * half_model, half_model), half_model)

    ff = gate.shape[1]
    pieces = 8
    piece_rows = ff // pieces
    far_core = (core + group) % 2
    far = (1 - side) * 2 + far_core

    def piece_at(n):
        return pl.ds(n * piece_rows, piece_rows)

    def down_far(n):
        return remote(
            down_hbm.at[piece_at(n), half_of(far_core)],
            down.at[2 + group, piece_at(n)],
            w_send.at[n],
            w_recv.at[n],
            tp=far,
        )

    def down_group(n, slot):
        return remote(
            down.at[slot, piece_at(n)],
            down.at[slot, piece_at(n)],
            y_send.at[n],
            y_recv.at[n],
            grp=1 - group,
        )

    def pass_down(n):
        down_far(n).wait_recv()
        down_group(n, 2 + group).start()

    down_partner = remote(
        down_hbm.at[:, half_of(1 - core)], down.at[1], d_send.at[0], d_recv.at[0], tp=partner
    )

    sources = (
        (keys_hbm, mixer_in.at[2]),
        (keys_narrow_hbm, mixer_in.at[3]),
        (values_hbm, mixer_in.at[4]),
        (values_narrow_hbm, mixer_in.at[5]),
        (queries_hbm, mixer_in.at[0]),
        (queries_narrow_hbm, mixer_in.at[1]),
        (out_wide_hbm, outs_in.at[0]),
        (out_narrow_hbm, outs_in.at[1]),
        (residual_hbm, residual),
        (gate_hbm, gate),
        (up_hbm, up),
        (down_hbm.at[:, half_of(core)], down.at[0]),
    )
    every_load = [
        pltpu.make_async_copy(src, dst, load_sem.at[n]) for n, (src, dst) in enumerate(sources)
    ]
    for load in every_load:
        load.start()
    loads = every_load[9:]
    queries, queries_narrow = mixer_in.at[0], mixer_in.at[1]
    keys, keys_narrow = mixer_in.at[2], mixer_in.at[3]
    values, values_narrow = mixer_in.at[4], mixer_in.at[5]
    out_wide, out_narrow = outs_in.at[0], outs_in.at[1]

    barrier = pltpu.get_barrier_semaphore()
    for target in (partner, across, diagonal_peer):
        pl.semaphore_signal(barrier, inc=1, device_id={"tp": target}, device_id_type=MESH)
    pl.semaphore_signal(barrier, inc=1, device_id={"grp": 1 - group}, device_id_type=MESH)

    @pl.loop(1, experts)
    def _(step):
        pl.semaphore_signal(barrier, inc=1, device_id={"sp": peer(step)}, device_id_type=MESH)
        pl.semaphore_signal(
            barrier, inc=1, device_id={"sp": peer(step), "tp": partner}, device_id_type=MESH
        )

    pl.semaphore_wait(barrier, 2 * experts + 2)
    early = pieces - 3
    for n in range(early):
        down_far(n).start()
    down_partner.start()

    length = queries.shape[0]
    rows_dev = residual.shape[0]
    fine_rows = fine.shape[2]
    coarse_rows = length // fine_rows
    at_coarse = pl.multiple_of(place * coarse_rows, coarse_rows)
    for narrow in range(2):
        cosine_fine, sine_fine = fine[narrow, 0], fine[narrow, 1]
        cosine_coarse = coarse[narrow, 0, pl.ds(at_coarse, coarse_rows), :]
        sine_coarse = coarse[narrow, 1, pl.ds(at_coarse, coarse_rows), :]
        for at in range(coarse_rows):
            cosine, sine_part = cosine_coarse[at : at + 1], sine_coarse[at : at + 1]
            span = slice(at * fine_rows, (at + 1) * fine_rows)
            turns[narrow, 0, span] = cosine * cosine_fine - sine_part * sine_fine
            turns[narrow, 1, span] = sine_part * cosine_fine + cosine * sine_fine

    def pieces_of(value):
        high = value.astype(jnp.bfloat16)
        rest = value - high.astype(jnp.float32)
        middle = rest.astype(jnp.bfloat16)
        low = (rest - middle.astype(jnp.float32)).astype(jnp.bfloat16)
        return high, middle, low

    row_at = lax.broadcasted_iota(jnp.int32, (128, 128), 0)
    lane_at = lax.broadcasted_iota(jnp.int32, (128, 128), 1)
    up_to = (row_at <= lane_at).astype(jnp.bfloat16)
    heads_wide, heads_narrow = decay_wide.shape[0], decay_narrow.shape[0]
    decays[...] = jnp.zeros_like(decays)
    decays[0:heads_wide, :] = decay_wide[...]
    decays[heads_wide : heads_wide + heads_narrow, :] = decay_narrow[...]
    running = jnp.zeros((8, 1), jnp.float32)
    for at in range(0, length, 128):
        within = running
        for piece in pieces_of(decays[:, at : at + 128]):
            within = within + jnp.dot(piece, up_to, preferred_element_type=jnp.float32)
        log_rows[:, at : at + 128] = within
        log_columns[at : at + 128, :] = within.T
        running = within[:, 127:128]

    for load in every_load[:4]:
        load.wait()
    lane = lax.broadcasted_iota(jnp.int32, (1, 128), 1)
    first = lane < HEAD_NARROW
    rows_128 = lax.broadcasted_iota(jnp.int32, (128, 128), 0)
    lanes_128 = lax.broadcasted_iota(jnp.int32, (128, 128), 1)
    diagonal = (rows_128 < HEAD_NARROW) == (lanes_128 < HEAD_NARROW)
    flips = []
    for width in (HEAD_WIDE, HEAD_NARROW):
        half_width = width // 2
        upper = lanes_128 % width >= half_width
        origin = jnp.where(upper, lanes_128 - half_width, lanes_128 + half_width)
        flips.append(
            jnp.where(rows_128 == origin, jnp.where(upper, 1.0, -1.0), 0.0).astype(jnp.bfloat16)
        )

    def unit_of(wide_ref, narrow_ref, unit):
        ref = narrow_ref if unit >= 2 else wide_ref
        return ref[:, unit % 2 * 128 : unit % 2 * 128 + 128]

    def per_lane(unit, table):
        if unit < 2:
            return table(unit)
        return jnp.where(first, table(2 * unit - 2), table(2 * unit - 1))

    def heads_of(unit):
        if unit < 2:
            return ((unit, None),)
        return ((2 * unit - 2, first), (2 * unit - 1, ~first))

    def masked(value, keep):
        return value if keep is None else jnp.where(keep, value, jnp.zeros_like(value))

    def swapped(value):
        return pltpu.roll(value, HEAD_NARROW, 1)

    def rotated(refs, unit):
        narrow = unit // 2
        value = unit_of(*refs, unit)
        flipped = jnp.dot(value, flips[narrow], preferred_element_type=jnp.float32)
        return value.astype(jnp.float32) * turns[narrow, 0] + flipped * turns[narrow, 1]

    packed = []
    for unit in range(4):
        narrow = unit // 2
        width = (HEAD_WIDE, HEAD_NARROW)[narrow]
        value = rotated((keys, keys_narrow), unit)
        turned[1, unit] = (value * width ** (-0.5)).astype(jnp.bfloat16)
        gap = per_lane(
            unit,
            lambda head: log_columns[length - 1 : length, head : head + 1]
            - log_columns[:, head : head + 1],
        )
        weighted = (turned[1, unit].astype(jnp.float32) * jnp.exp(gap)).astype(jnp.bfloat16)
        state = lax.dot_general(
            weighted,
            unit_of(values, values_narrow, unit),
            (((0,), (0,)), ((), ())),
            preferred_element_type=jnp.float32,
        )
        last = log_columns[length - 1 : length, :]
        total_row = per_lane(
            unit, lambda head: jnp.broadcast_to(last[:, head : head + 1], (1, 128))
        )
        if unit == 3:
            state, total_row = swapped(state), swapped(total_row)
        packed.append(state)
        local_total[unit : unit + 1, :] = total_row
    for unit in range(4, 8):
        local_total[unit : unit + 1, :] = jnp.zeros((1, 128), jnp.float32)
    local_state[0] = packed[0].astype(jnp.bfloat16)
    local_state[1] = packed[1].astype(jnp.bfloat16)
    local_state[2] = jnp.where(diagonal, packed[2], packed[3]).astype(jnp.bfloat16)

    def send_state(source, target):
        return remote(
            local_state, states.at[source], s_send.at[target], s_recv.at[source], sp=target
        )

    def send_total(source, target):
        return remote(
            local_total, totals.at[source], t_send.at[target], t_recv.at[source], sp=target
        )

    @pl.loop(place + 1, experts)
    def _(target):
        send_state(place, target).start()
        send_total(place, target).start()

    named = lax.broadcasted_iota(jnp.int32, (slot_rows.shape[0], rows_dev), 0)
    hits = (routes[0:1, :] == named) | (routes[1:2, :] == named)
    earlier = lax.broadcasted_iota(jnp.int32, (rows_dev, rows_dev), 0) < lax.broadcasted_iota(
        jnp.int32, (rows_dev, rows_dev), 1
    )
    rank = jnp.dot(
        hits.astype(jnp.bfloat16),
        earlier.astype(jnp.bfloat16),
        preferred_element_type=jnp.float32,
    )
    slot_rows[...] = jnp.where(hits, rank, -1.0)
    slot_columns[...] = slot_rows[...].T
    weight_columns[...] = (
        jnp.where(routes[0:1, :] == named, weights[0:1, :], 0.0)
        + jnp.where(routes[1:2, :] == named, weights[1:2, :], 0.0)
    ).T
    for load in every_load[4:6]:
        load.wait()
    for unit in range(4):
        turned[0, unit] = rotated((queries, queries_narrow), unit).astype(jnp.bfloat16)

    tile = min(length, 256)
    for unit in range(4):
        value = unit_of(values, values_narrow, unit)
        for start in range(0, length, tile):
            stop = start + tile
            steps = lax.broadcasted_iota(jnp.int32, (tile, stop), 0) + start
            causal = steps >= lax.broadcasted_iota(jnp.int32, (tile, stop), 1)
            total = jnp.zeros((tile, 128), jnp.float32)
            for head, keep in heads_of(unit):
                gaps = log_columns[start:stop, head : head + 1] - log_rows[head : head + 1, :stop]
                decay_grid = jnp.exp(jnp.where(causal, gaps, -1e30))
                scores = lax.dot_general(
                    masked(turned[0, unit, start:stop], keep),
                    turned[1, unit, :stop],
                    (((1,), (1,)), ((), ())),
                    preferred_element_type=jnp.float32,
                )
                total += jnp.dot(
                    (scores * decay_grid).astype(jnp.bfloat16),
                    masked(value[:stop], keep),
                    preferred_element_type=jnp.float32,
                )
            inner[unit, start:stop] = total

    def join(source, carried):
        send_state(source, source).wait_recv()
        send_total(source, source).wait_recv()
        fade = jnp.exp(totals[source])
        fade_narrow = jnp.where(diagonal, fade[2:3], fade[3:4])
        return (
            carried[0] * fade[0:1] + states[source, 0].astype(jnp.float32),
            carried[1] * fade[1:2] + states[source, 1].astype(jnp.float32),
            carried[2] * fade_narrow + states[source, 2].astype(jnp.float32),
        )

    pass_down(0)
    nothing = jnp.zeros((128, 128), jnp.float32)
    carried = lax.fori_loop(0, place, join, (nothing, nothing, nothing))
    for unit in range(4):
        state = carried[min(unit, 2)]
        if unit == 2:
            state = jnp.where(diagonal, state, 0.0)
        if unit == 3:
            state = swapped(jnp.where(diagonal, 0.0, state))
        fade = jnp.exp(per_lane(unit, lambda head: log_columns[:, head : head + 1]))
        value = inner[unit] + fade * jnp.dot(
            turned[0, unit], state.astype(jnp.bfloat16), preferred_element_type=jnp.float32
        )

        def mean_of(value):
            if unit < 2:
                return jnp.mean(value, axis=-1, keepdims=True)
            low = jnp.sum(masked(value, first), axis=-1, keepdims=True)
            high = jnp.sum(masked(value, ~first), axis=-1, keepdims=True)
            return jnp.where(first, low, high) / HEAD_NARROW

        value = value - mean_of(value)
        spread = mean_of(value * value)
        mixed[:, unit * 128 : unit * 128 + 128] = (value * lax.rsqrt(spread + norm_eps)).astype(
            jnp.bfloat16
        )

    columns = 4
    width = model_width // columns

    def to_partner(n, at):
        where = (n, slice(None), pl.ds(at * width, width))
        return remote(
            part.at[where], part_in.at[where], a_send.at[n, at], a_recv.at[n, at], tp=partner
        )

    def to_across(at):
        where = (slice(None), pl.ds(at * width, width))
        return remote(
            cross.at[where], cross_in.at[where], a_send.at[2, at], a_recv.at[2, at], tp=across
        )

    for load in every_load[6:9]:
        load.wait()

    def projected(target, at):
        picked = mixed[pl.ds(pl.multiple_of(target * rows_dev, rows_dev), rows_dev), :]
        span = slice(at * width, (at + 1) * width)
        return jnp.dot(
            picked[:, :256], out_wide[:, span], preferred_element_type=jnp.float32
        ) + jnp.dot(picked[:, 256:], out_narrow[:, span], preferred_element_type=jnp.float32)

    for at in range(columns):
        span = slice(at * width, (at + 1) * width)
        part[0, :, span] = projected(diagonal_peer, at).astype(jnp.bfloat16)
        to_partner(0, at).start()
    for at in range(columns):
        span = slice(at * width, (at + 1) * width)
        value = projected(across, at)
        to_partner(0, at).wait_recv()
        cross[:, span] = (value + part_in[0, :, span].astype(jnp.float32)).astype(jnp.bfloat16)
        to_across(at).start()
    pass_down(1)
    for at in range(columns):
        span = slice(at * width, (at + 1) * width)
        part[1, :, span] = projected(partner, at).astype(jnp.bfloat16)
        to_partner(1, at).start()
    for at in range(columns):
        span = slice(at * width, (at + 1) * width)
        value = residual[:, span].astype(jnp.float32) + projected(mine, at)
        to_partner(1, at).wait_recv()
        hidden_state[:, span] = value + part_in[1, :, span].astype(jnp.float32)
    for n in range(2, early):
        pass_down(n)
    for at in range(columns):
        to_across(at).wait_recv()
    total = hidden_state[...] + cross_in[...].astype(jnp.float32)
    hidden_state[...] = total
    scale_row = lax.rsqrt(jnp.mean(total * total, axis=-1, keepdims=True) + norm_eps)
    normed = (total * scale_row * gain[...]).astype(jnp.bfloat16)

    slot_at = lax.broadcasted_iota(jnp.int32, (capacity, rows_dev), 0).astype(jnp.float32)

    def slots(expert):
        scatter = (slot_rows[pl.ds(expert, 1), :] == slot_at).astype(jnp.bfloat16)
        return jnp.dot(scatter, normed, preferred_element_type=jnp.float32).astype(jnp.bfloat16)

    shares = 2 if capacity % 32 == 0 else 1
    share = capacity // shares

    def share_at(n):
        return pl.ds(n * share, share)

    def dispatch(expert, n):
        return remote(
            send.at[expert, share_at(n)],
            rows.at[place, mine, share_at(n)],
            z_send.at[expert, n],
            z_recv.at[place, n],
            sp=expert,
        )

    def arrived(source, n):
        return remote(
            send.at[source, share_at(n)],
            rows.at[source, mine, share_at(n)],
            z_send.at[source, n],
            z_recv.at[source, n],
            sp=source,
        )

    def forward_across(source, n):
        return remote(
            rows.at[source, mine, share_at(n)],
            rows.at[source, mine, share_at(n)],
            x_send.at[source, n],
            x_recv.at[source, n],
            tp=across,
        )

    def forward_partner(source, n):
        return remote(
            rows.at[source, mine, share_at(n)],
            rows.at[source, mine, share_at(n)],
            p_send.at[source, n],
            p_recv.at[source, n],
            tp=partner,
        )

    def pass_across(source, n):
        return remote(
            rows.at[source, across, share_at(n)],
            rows.at[source, across, share_at(n)],
            p_send.at[source, shares + n],
            p_recv.at[source, shares + n],
            tp=partner,
        )

    def forward(source, n):
        forward_across(source, n).start()
        forward_partner(source, n).start()

    def hidden_across(source):
        return remote(
            hidden_own.at[source, 1 - side],
            hidden_in.at[source, 1],
            h_send.at[source, 1],
            h_recv.at[source, 1],
            tp=across,
        )

    def hidden_partner(source):
        return remote(
            hidden_own.at[source, side],
            hidden_in.at[source, 0],
            h_send.at[source, 0],
            h_recv.at[source, 0],
            tp=partner,
        )

    def hidden_forward(source):
        return remote(
            hidden_in.at[source, 1],
            hidden_in.at[source, 2],
            h_send.at[source, 2],
            h_recv.at[source, 2],
            tp=partner,
        )

    def give_back(source):
        return remote(
            result.at[source, core],
            returned.at[place, core],
            r_send.at[source, 0],
            r_recv.at[place, core],
            sp=source,
        )

    def give_partner(source):
        return remote(
            result.at[source, 1 - core],
            returned.at[place, core],
            r_send.at[source, 1],
            r_recv.at[place, core],
            sp=source,
            tp=partner,
        )

    def came_back(expert, which):
        return remote(
            result.at[expert, 0],
            returned.at[expert, which],
            r_send.at[expert, 0],
            r_recv.at[expert, which],
            sp=expert,
        )

    @pl.loop(1, experts)
    def _(step):
        expert = peer(step)
        send[expert] = slots(expert)
        for n in range(shares):
            dispatch(expert, n).start()

    rows[place, mine] = slots(place)

    for load in loads:
        load.wait()

    ff_step = min(ff, 256)
    out_step = min(half_model, 512)

    def spread(source):
        hidden_across(source).wait_recv()
        hidden_forward(source).start()

    def finish(source):
        hidden_partner(source).wait_recv()
        hidden_forward(source).wait_recv()
        for at in range(0, half_model, out_step):
            span = slice(at, at + out_step)
            value = jnp.dot(
                hidden_own[source, side], down[0, :, span], preferred_element_type=jnp.float32
            )
            for n in range(3):
                value = value + jnp.dot(
                    hidden_in[source, n], down[n + 1, :, span], preferred_element_type=jnp.float32
                )
            value = value.astype(jnp.bfloat16)
            for n in range(2):
                result[source, n, :, span] = value[n * capacity : (n + 1) * capacity]

        @pl.when(source == place)
        def _():
            returned[place, core] = result[place, core]
            remote(
                result.at[place, 1 - core],
                returned.at[place, core],
                r_send.at[place, 1],
                r_recv.at[place, core],
                tp=partner,
            ).start()

        @pl.when(source != place)
        def _():
            give_back(source).start()
            give_partner(source).start()

    def take(step):
        later = peer(step)
        for n in range(shares):
            arrived(later, n).wait_recv()
            forward(later, n)

    def expand(source):
        for n in range(shares):
            forward_across(source, n).wait_recv()
            pass_across(source, n).start()
        for n in range(shares):
            forward_partner(source, n).wait_recv()
            pass_across(source, n).wait_recv()
        block = rows[source].reshape(4 * capacity, model_width)
        for at in range(0, ff, ff_step):
            span = slice(at, at + ff_step)
            gate_pre = jnp.dot(block, gate[:, span], preferred_element_type=jnp.float32)
            up_pre = jnp.dot(block, up[:, span], preferred_element_type=jnp.float32)
            value = activate(gate_pre, up_pre).astype(jnp.bfloat16)
            for n in range(2):
                hidden_own[source, n, :, span] = value[2 * n * capacity : 2 * (n + 1) * capacity]

    def swap_hidden(source):
        hidden_across(source).start()
        hidden_partner(source).start()

    if short:
        for n in range(early, pieces):
            down_far(n).start()
        take(1)
        take(2)
        expand(peer(1))
        for n in range(early, pieces):
            pass_down(n)
        swap_hidden(peer(1))
        expand(peer(2))
        swap_hidden(peer(2))
        take(3)
        for n in range(shares):
            forward(place, n)
        down_partner.wait_recv()
        for n in range(pieces):
            down_group(n, 3 - group).wait_recv()
        spread(peer(2))
        finish(peer(2))
        spread(peer(1))
        finish(peer(1))
        expand(peer(3))
        swap_hidden(peer(3))
        expand(place)
        swap_hidden(place)
        spread(peer(3))
        finish(peer(3))
        spread(place)
        finish(place)
    else:
        for n in range(shares):
            forward(place, n)
        take(1)
        for n in range(early, pieces):
            down_far(n).start()
        expand(place)

        @pl.loop(1, experts)
        def _(step):
            source = peer(step)
            expand(source)
            swap_hidden(source)

            @pl.when(step == 1)
            def _():
                for n in range(early, pieces):
                    pass_down(n)

            @pl.when(step + 1 < experts)
            def _():
                take(step + 1)

            @pl.when(step + 1 == experts)
            def _():
                swap_hidden(place)

            @pl.when(step == 1)
            def _():
                down_partner.wait_recv()
                for n in range(pieces):
                    down_group(n, 3 - group).wait_recv()

            spread(source)
            finish(source)

        spread(place)
        finish(place)

    slot_lane = lax.broadcasted_iota(jnp.int32, (rows_dev, capacity), 1).astype(jnp.float32)
    name_lane = lax.broadcasted_iota(jnp.int32, slot_columns.shape, 1)

    def column_of(table, expert):
        kept = jnp.where(name_lane == expert, table[...], 0.0)
        return jnp.sum(kept, axis=1, keepdims=True)

    def add_expert(expert):
        pick = (column_of(slot_columns, expert) == slot_lane).astype(jnp.bfloat16)
        weight = column_of(weight_columns, expert)
        for n in range(2):
            span = slice(n * half_model, (n + 1) * half_model)
            hidden_state[:, span] += weight * jnp.dot(
                pick, returned[expert, n], preferred_element_type=jnp.float32
            )

    came_back(place, 1 - core).wait_recv()
    add_expert(place)

    @pl.loop(1, experts)
    def _(step):
        expert = peer(step)
        came_back(expert, 0).wait_recv()
        came_back(expert, 1).wait_recv()
        add_expert(expert)

    total = hidden_state[...]
    output[...] = total.astype(output.dtype)

    @pl.loop(place + 1, experts)
    def _(target):
        send_state(place, target).wait_send()
        send_total(place, target).wait_send()

    for at in range(columns):
        to_partner(0, at).wait_send()
        to_partner(1, at).wait_send()
        to_across(at).wait_send()
    for n in range(pieces):
        down_far(n).wait_send()
        down_group(n, 2 + group).wait_send()
    down_partner.wait_send()

    @pl.loop(0, experts)
    def _(step):
        source = peer(step)
        for n in range(shares):
            forward_across(source, n).wait_send()
            forward_partner(source, n).wait_send()
            pass_across(source, n).wait_send()
        hidden_across(source).wait_send()
        hidden_partner(source).wait_send()
        hidden_forward(source).wait_send()
        give_partner(source).wait_send()

        @pl.when(step >= 1)
        def _():
            for n in range(shares):
                dispatch(source, n).wait_send()
            give_back(source).wait_send()


FINE_ROWS = 32


def rotary_tables(steps):
    grids = []
    for at in (np.arange(0, steps, FINE_ROWS), np.arange(FINE_ROWS)):
        grid = []
        for width in (HEAD_WIDE, HEAD_NARROW):
            half_width = width // 2
            inverse = np.float32(rotary_base) ** (
                -np.arange(half_width, dtype=np.float32) / np.float32(half_width)
            )
            angles = at[:, None] * np.tile(inverse.astype(np.float64), 128 // half_width)
            grid.append(np.stack([np.cos(angles), np.sin(angles)]))
        grids.append(np.stack(grid).astype(np.float32))
    return grids


def layer(mixer_inputs, decays, outs, residual, norm_gain, routes, route_weights, gate, up, down):
    experts = lax.axis_size("sp")
    rows_dev, model_width = residual.shape
    length = mixer_inputs[0].shape[0]
    ff = gate.shape[1]
    limit = max(TOP_K, 3 * rows_dev * TOP_K // (2 * experts))
    capacity = -(-limit // 16) * 16
    named = -(-experts // 8) * 8
    coarse, fine = rotary_tables(experts * length)
    bf16 = jnp.bfloat16
    block = (capacity, model_width)
    dma = pltpu.SemaphoreType.DMA
    vmem = pl.BlockSpec(memory_space=pltpu.VMEM)
    anywhere = pl.BlockSpec(memory_space=pl.ANY)
    return pl.pallas_call(
        functools.partial(tail_kernel, experts, capacity),
        out_shape=jax.ShapeDtypeStruct((rows_dev, model_width), bf16),
        in_specs=[anywhere] * 12 + [vmem] * 7,
        out_specs=vmem,
        scratch_shapes=[
            pltpu.VMEM((6, *mixer_inputs[0].shape), bf16),
            pltpu.VMEM((2, *outs[0].shape), bf16),
            pltpu.VMEM((rows_dev, model_width), bf16),
            pltpu.VMEM((model_width, ff), bf16),
            pltpu.VMEM((model_width, ff), bf16),
            pltpu.VMEM((4, ff, model_width // 2), bf16),
            pltpu.VMEM((8, length), jnp.float32),
            pltpu.VMEM((8, length), jnp.float32),
            pltpu.VMEM((length, 8), jnp.float32),
            pltpu.VMEM((2, 2, length, 128), jnp.float32),
            pltpu.VMEM((named, rows_dev), jnp.float32),
            pltpu.VMEM((rows_dev, named), jnp.float32),
            pltpu.VMEM((rows_dev, named), jnp.float32),
            pltpu.VMEM((4, rows_dev, model_width), bf16),
            pltpu.VMEM((2, rows_dev, model_width), bf16),
            pltpu.VMEM((rows_dev, model_width), bf16),
            pltpu.VMEM((rows_dev, model_width), bf16),
            pltpu.VMEM((rows_dev, model_width), jnp.float32),
            pltpu.VMEM((experts, *block), bf16),
            pltpu.VMEM((experts, 4, *block), bf16),
            pltpu.VMEM((experts, 2, 2 * capacity, ff), bf16),
            pltpu.VMEM((experts, 3, 2 * capacity, ff), bf16),
            pltpu.VMEM((experts, 2, capacity, model_width // 2), bf16),
            pltpu.VMEM((experts, 2, capacity, model_width // 2), bf16),
            pltpu.VMEM((length, 512), bf16),
            pltpu.VMEM((4, length, 128), jnp.float32),
            pltpu.VMEM((2, 4, length, 128), bf16),
            pltpu.VMEM((3, 128, 128), bf16),
            pltpu.VMEM((8, 128), jnp.float32),
            pltpu.VMEM((experts, 3, 128, 128), bf16),
            pltpu.VMEM((experts, 8, 128), jnp.float32),
            dma((12,)),
            dma((experts,)),
            dma((experts,)),
            dma((experts,)),
            dma((experts,)),
            dma((3, 4)),
            dma((3, 4)),
            dma((experts, 2)),
            dma((experts, 2)),
            dma((experts, 2)),
            dma((experts, 2)),
            dma((experts, 4)),
            dma((experts, 4)),
            dma((experts, 3)),
            dma((experts, 3)),
            dma((experts, 2)),
            dma((experts, 2)),
            dma((8,)),
            dma((8,)),
            dma((8,)),
            dma((8,)),
            dma((1,)),
            dma((1,)),
        ],
        compiler_params=pltpu.CompilerParams(
            collective_id=1, has_side_effects=True, vmem_limit_bytes=60 * 1024 * 1024
        ),
    )(
        *mixer_inputs,
        *outs,
        residual,
        gate,
        up,
        down,
        *decays,
        coarse,
        fine,
        norm_gain.reshape(1, model_width),
        routes.T,
        route_weights.T,
    )


def body(
    query_wide,
    key_wide,
    value_wide,
    decay_wide,
    query_narrow,
    key_narrow,
    value_narrow,
    decay_narrow,
    residual,
    out_wide,
    out_narrow,
    norm_gain,
    routes,
    route_weights,
    expert_gate,
    expert_up,
    expert_down,
):
    return layer(
        (
            query_wide,
            query_narrow,
            key_wide,
            key_narrow,
            value_wide,
            value_narrow,
        ),
        (decay_wide.T, decay_narrow.T),
        (out_wide, out_narrow),
        residual,
        norm_gain,
        routes,
        route_weights,
        expert_gate[0],
        expert_up[0],
        expert_down[0],
    )


def solution(mesh):
    placed = (
        P(("grp", "sp"), "tp"),
        P(("grp", "sp"), "tp"),
        P(("grp", "sp"), "tp"),
        P(("grp", "sp"), "tp"),
        P(("grp", "sp"), "tp"),
        P(("grp", "sp"), "tp"),
        P(("grp", "sp"), "tp"),
        P(("grp", "sp"), "tp"),
        P(("grp", "sp", "tp"), None),
        P("tp", None),
        P("tp", None),
        P(),
        P(("grp", "sp", "tp"), None),
        P(("grp", "sp", "tp"), None),
        P("sp", None, "tp"),
        P("sp", None, "tp"),
        P("sp", "tp", None),
    )
    return jax.shard_map(
        body, mesh=mesh, in_specs=placed, out_specs=P(("grp", "sp", "tp"), None), check_vma=False
    )
```

```python
import functools

import jax
import jax.numpy as jnp
import numpy as np
from jax import lax
from jax.experimental import pallas as pl
from jax.experimental.pallas import tpu as pltpu
from jax.sharding import PartitionSpec as P

HEAD_WIDE = 128
HEAD_NARROW = 64
TOP_K = 2


norm_eps = 1e-05
clamp_limit = 7.0
swish_alpha = 1.702
rotary_base = 10000.0


def activate(gate_pre, up_pre):
    gate_clip = jnp.minimum(gate_pre, clamp_limit)
    up_clip = jnp.clip(up_pre, -clamp_limit, clamp_limit)
    return gate_clip * jax.nn.sigmoid(swish_alpha * gate_clip) * (up_clip + 1.0)


MESH = pl.DeviceIdType.MESH


def tail_kernel(
    experts,
    capacity,
    queries_hbm,
    queries_narrow_hbm,
    keys_hbm,
    keys_narrow_hbm,
    values_hbm,
    values_narrow_hbm,
    out_wide_hbm,
    out_narrow_hbm,
    residual_hbm,
    gate_hbm,
    up_hbm,
    down_hbm,
    decay_wide,
    decay_narrow,
    coarse,
    fine,
    gain,
    routes,
    weights,
    output,
    mixer_in,
    outs_in,
    residual,
    gate,
    up,
    down,
    decays,
    log_rows,
    log_columns,
    turns,
    slot_rows,
    slot_columns,
    weight_columns,
    part,
    part_in,
    cross,
    cross_in,
    hidden_state,
    send,
    rows,
    hidden_own,
    hidden_in,
    result,
    returned,
    mixed,
    inner,
    turned,
    local_state,
    local_total,
    states,
    totals,
    load_sem,
    s_send,
    s_recv,
    t_send,
    t_recv,
    a_send,
    a_recv,
    z_send,
    z_recv,
    x_send,
    x_recv,
    p_send,
    p_recv,
    h_send,
    h_recv,
    r_send,
    r_recv,
    w_send,
    w_recv,
    y_send,
    y_recv,
    d_send,
    d_recv,
):
    place = lax.axis_index("sp")
    mine = lax.axis_index("tp")
    core, side = mine % 2, mine // 2
    partner = side * 2 + (1 - core)
    across = (1 - side) * 2 + core
    diagonal_peer = (1 - side) * 2 + 1 - core
    group = lax.axis_index("grp")
    model_width = residual.shape[1]
    half_model = model_width // 2

    def remote(src, dst, send_sem, recv_sem, **where):
        return pltpu.make_async_remote_copy(
            src_ref=src,
            dst_ref=dst,
            send_sem=send_sem,
            recv_sem=recv_sem,
            device_id=where,
            device_id_type=MESH,
        )

    order = (0, 1, 2, 3)
    short = experts == len(order)

    def peer(step):
        if short and isinstance(step, int):
            return place ^ order[step]
        return lax.rem(place + step, experts) if experts & (experts - 1) else place ^ step

    def half_of(which):
        return pl.ds(pl.multiple_of(which * half_model, half_model), half_model)

    ff = gate.shape[1]
    pieces = 8
    piece_rows = ff // pieces
    far_core = (core + group) % 2
    far = (1 - side) * 2 + far_core

    def piece_at(n):
        return pl.ds(n * piece_rows, piece_rows)

    def down_far(n):
        return remote(
            down_hbm.at[piece_at(n), half_of(far_core)],
            down.at[2 + group, piece_at(n)],
            w_send.at[n],
            w_recv.at[n],
            tp=far,
        )

    def down_group(n, slot):
        return remote(
            down.at[slot, piece_at(n)],
            down.at[slot, piece_at(n)],
            y_send.at[n],
            y_recv.at[n],
            grp=1 - group,
        )

    def pass_down(n):
        down_far(n).wait_recv()
        down_group(n, 2 + group).start()

    down_partner = remote(
        down_hbm.at[:, half_of(1 - core)], down.at[1], d_send.at[0], d_recv.at[0], tp=partner
    )

    sources = (
        (keys_hbm, mixer_in.at[2]),
        (keys_narrow_hbm, mixer_in.at[3]),
        (values_hbm, mixer_in.at[4]),
        (values_narrow_hbm, mixer_in.at[5]),
        (queries_hbm, mixer_in.at[0]),
        (queries_narrow_hbm, mixer_in.at[1]),
        (out_wide_hbm, outs_in.at[0]),
        (out_narrow_hbm, outs_in.at[1]),
        (residual_hbm, residual),
        (gate_hbm, gate),
        (up_hbm, up),
        (down_hbm.at[:, half_of(core)], down.at[0]),
    )
    every_load = [
        pltpu.make_async_copy(src, dst, load_sem.at[n]) for n, (src, dst) in enumerate(sources)
    ]
    for load in every_load:
        load.start()
    loads = every_load[9:]
    queries, queries_narrow = mixer_in.at[0], mixer_in.at[1]
    keys, keys_narrow = mixer_in.at[2], mixer_in.at[3]
    values, values_narrow = mixer_in.at[4], mixer_in.at[5]
    out_wide, out_narrow = outs_in.at[0], outs_in.at[1]

    barrier = pltpu.get_barrier_semaphore()
    for target in (partner, across, diagonal_peer):
        pl.semaphore_signal(barrier, inc=1, device_id={"tp": target}, device_id_type=MESH)
    pl.semaphore_signal(barrier, inc=1, device_id={"grp": 1 - group}, device_id_type=MESH)

    @pl.loop(1, experts)
    def _(step):
        pl.semaphore_signal(barrier, inc=1, device_id={"sp": peer(step)}, device_id_type=MESH)
        pl.semaphore_signal(
            barrier, inc=1, device_id={"sp": peer(step), "tp": partner}, device_id_type=MESH
        )

    pl.semaphore_wait(barrier, 2 * experts + 2)
    early = pieces - 3
    for n in range(early):
        down_far(n).start()
    down_partner.start()

    length = queries.shape[0]
    rows_dev = residual.shape[0]
    fine_rows = fine.shape[2]
    coarse_rows = length // fine_rows
    at_coarse = pl.multiple_of(place * coarse_rows, coarse_rows)
    for narrow in range(2):
        cosine_fine, sine_fine = fine[narrow, 0], fine[narrow, 1]
        cosine_coarse = coarse[narrow, 0, pl.ds(at_coarse, coarse_rows), :]
        sine_coarse = coarse[narrow, 1, pl.ds(at_coarse, coarse_rows), :]
        for at in range(coarse_rows):
            cosine, sine_part = cosine_coarse[at : at + 1], sine_coarse[at : at + 1]
            span = slice(at * fine_rows, (at + 1) * fine_rows)
            turns[narrow, 0, span] = cosine * cosine_fine - sine_part * sine_fine
            turns[narrow, 1, span] = sine_part * cosine_fine + cosine * sine_fine

    def pieces_of(value):
        high = value.astype(jnp.bfloat16)
        rest = value - high.astype(jnp.float32)
        middle = rest.astype(jnp.bfloat16)
        low = (rest - middle.astype(jnp.float32)).astype(jnp.bfloat16)
        return high, middle, low

    row_at = lax.broadcasted_iota(jnp.int32, (128, 128), 0)
    lane_at = lax.broadcasted_iota(jnp.int32, (128, 128), 1)
    up_to = (row_at <= lane_at).astype(jnp.bfloat16)
    heads_wide, heads_narrow = decay_wide.shape[0], decay_narrow.shape[0]
    decays[...] = jnp.zeros_like(decays)
    decays[0:heads_wide, :] = decay_wide[...]
    decays[heads_wide : heads_wide + heads_narrow, :] = decay_narrow[...]
    running = jnp.zeros((8, 1), jnp.float32)
    for at in range(0, length, 128):
        within = running
        for piece in pieces_of(decays[:, at : at + 128]):
            within = within + jnp.dot(piece, up_to, preferred_element_type=jnp.float32)
        log_rows[:, at : at + 128] = within
        log_columns[at : at + 128, :] = within.T
        running = within[:, 127:128]

    for load in every_load[:4]:
        load.wait()
    lane = lax.broadcasted_iota(jnp.int32, (1, 128), 1)
    first = lane < HEAD_NARROW
    rows_128 = lax.broadcasted_iota(jnp.int32, (128, 128), 0)
    lanes_128 = lax.broadcasted_iota(jnp.int32, (128, 128), 1)
    diagonal = (rows_128 < HEAD_NARROW) == (lanes_128 < HEAD_NARROW)
    flips = []
    for width in (HEAD_WIDE, HEAD_NARROW):
        half_width = width // 2
        upper = lanes_128 % width >= half_width
        origin = jnp.where(upper, lanes_128 - half_width, lanes_128 + half_width)
        flips.append(
            jnp.where(rows_128 == origin, jnp.where(upper, 1.0, -1.0), 0.0).astype(jnp.bfloat16)
        )

    def unit_of(wide_ref, narrow_ref, unit):
        ref = narrow_ref if unit >= 2 else wide_ref
        return ref[:, unit % 2 * 128 : unit % 2 * 128 + 128]

    def per_lane(unit, table):
        if unit < 2:
            return table(unit)
        return jnp.where(first, table(2 * unit - 2), table(2 * unit - 1))

    def heads_of(unit):
        if unit < 2:
            return ((unit, None),)
        return ((2 * unit - 2, first), (2 * unit - 1, ~first))

    def masked(value, keep):
        return value if keep is None else jnp.where(keep, value, jnp.zeros_like(value))

    def swapped(value):
        return pltpu.roll(value, HEAD_NARROW, 1)

    def rotated(refs, unit):
        narrow = unit // 2
        value = unit_of(*refs, unit)
        flipped = jnp.dot(value, flips[narrow], preferred_element_type=jnp.float32)
        return value.astype(jnp.float32) * turns[narrow, 0] + flipped * turns[narrow, 1]

    packed = []
    for unit in range(4):
        narrow = unit // 2
        width = (HEAD_WIDE, HEAD_NARROW)[narrow]
        value = rotated((keys, keys_narrow), unit)
        turned[1, unit] = (value * width ** (-0.5)).astype(jnp.bfloat16)
        gap = per_lane(
            unit,
            lambda head: log_columns[length - 1 : length, head : head + 1]
            - log_columns[:, head : head + 1],
        )
        weighted = (turned[1, unit].astype(jnp.float32) * jnp.exp(gap)).astype(jnp.bfloat16)
        state = lax.dot_general(
            weighted,
            unit_of(values, values_narrow, unit),
            (((0,), (0,)), ((), ())),
            preferred_element_type=jnp.float32,
        )
        last = log_columns[length - 1 : length, :]
        total_row = per_lane(
            unit, lambda head: jnp.broadcast_to(last[:, head : head + 1], (1, 128))
        )
        if unit == 3:
            state, total_row = swapped(state), swapped(total_row)
        packed.append(state)
        local_total[unit : unit + 1, :] = total_row
    for unit in range(4, 8):
        local_total[unit : unit + 1, :] = jnp.zeros((1, 128), jnp.float32)
    local_state[0] = packed[0].astype(jnp.bfloat16)
    local_state[1] = packed[1].astype(jnp.bfloat16)
    local_state[2] = jnp.where(diagonal, packed[2], packed[3]).astype(jnp.bfloat16)

    def send_state(source, target):
        return remote(
            local_state, states.at[source], s_send.at[target], s_recv.at[source], sp=target
        )

    def send_total(source, target):
        return remote(
            local_total, totals.at[source], t_send.at[target], t_recv.at[source], sp=target
        )

    @pl.loop(place + 1, experts)
    def _(target):
        send_state(place, target).start()
        send_total(place, target).start()

    named = lax.broadcasted_iota(jnp.int32, (slot_rows.shape[0], rows_dev), 0)
    hits = (routes[0:1, :] == named) | (routes[1:2, :] == named)
    earlier = lax.broadcasted_iota(jnp.int32, (rows_dev, rows_dev), 0) < lax.broadcasted_iota(
        jnp.int32, (rows_dev, rows_dev), 1
    )
    rank = jnp.dot(
        hits.astype(jnp.bfloat16),
        earlier.astype(jnp.bfloat16),
        preferred_element_type=jnp.float32,
    )
    slot_rows[...] = jnp.where(hits, rank, -1.0)
    slot_columns[...] = slot_rows[...].T
    weight_columns[...] = (
        jnp.where(routes[0:1, :] == named, weights[0:1, :], 0.0)
        + jnp.where(routes[1:2, :] == named, weights[1:2, :], 0.0)
    ).T
    for load in every_load[4:6]:
        load.wait()
    for unit in range(4):
        turned[0, unit] = rotated((queries, queries_narrow), unit).astype(jnp.bfloat16)

    tile = min(length, 256)
    for unit in range(4):
        value = unit_of(values, values_narrow, unit)
        for start in range(0, length, tile):
            stop = start + tile
            steps = lax.broadcasted_iota(jnp.int32, (tile, stop), 0) + start
            causal = steps >= lax.broadcasted_iota(jnp.int32, (tile, stop), 1)
            total = jnp.zeros((tile, 128), jnp.float32)
            for head, keep in heads_of(unit):
                gaps = log_columns[start:stop, head : head + 1] - log_rows[head : head + 1, :stop]
                decay_grid = jnp.exp(jnp.where(causal, gaps, -1e30))
                scores = lax.dot_general(
                    masked(turned[0, unit, start:stop], keep),
                    turned[1, unit, :stop],
                    (((1,), (1,)), ((), ())),
                    preferred_element_type=jnp.float32,
                )
                total += jnp.dot(
                    (scores * decay_grid).astype(jnp.bfloat16),
                    masked(value[:stop], keep),
                    preferred_element_type=jnp.float32,
                )
            inner[unit, start:stop] = total

    def join(source, carried):
        send_state(source, source).wait_recv()
        send_total(source, source).wait_recv()
        fade = jnp.exp(totals[source])
        fade_narrow = jnp.where(diagonal, fade[2:3], fade[3:4])
        return (
            carried[0] * fade[0:1] + states[source, 0].astype(jnp.float32),
            carried[1] * fade[1:2] + states[source, 1].astype(jnp.float32),
            carried[2] * fade_narrow + states[source, 2].astype(jnp.float32),
        )

    pass_down(0)
    nothing = jnp.zeros((128, 128), jnp.float32)
    carried = lax.fori_loop(0, place, join, (nothing, nothing, nothing))
    for unit in range(4):
        state = carried[min(unit, 2)]
        if unit == 2:
            state = jnp.where(diagonal, state, 0.0)
        if unit == 3:
            state = swapped(jnp.where(diagonal, 0.0, state))
        fade = jnp.exp(per_lane(unit, lambda head: log_columns[:, head : head + 1]))
        value = inner[unit] + fade * jnp.dot(
            turned[0, unit], state.astype(jnp.bfloat16), preferred_element_type=jnp.float32
        )

        def mean_of(value):
            if unit < 2:
                return jnp.mean(value, axis=-1, keepdims=True)
            low = jnp.sum(masked(value, first), axis=-1, keepdims=True)
            high = jnp.sum(masked(value, ~first), axis=-1, keepdims=True)
            return jnp.where(first, low, high) / HEAD_NARROW

        value = value - mean_of(value)
        spread = mean_of(value * value)
        mixed[:, unit * 128 : unit * 128 + 128] = (value * lax.rsqrt(spread + norm_eps)).astype(
            jnp.bfloat16
        )

    columns = 4
    width = model_width // columns

    def to_partner(n, at):
        where = (n, slice(None), pl.ds(at * width, width))
        return remote(
            part.at[where], part_in.at[where], a_send.at[n, at], a_recv.at[n, at], tp=partner
        )

    def to_across(at):
        where = (slice(None), pl.ds(at * width, width))
        return remote(
            cross.at[where], cross_in.at[where], a_send.at[2, at], a_recv.at[2, at], tp=across
        )

    for load in every_load[6:9]:
        load.wait()

    def projected(target, at):
        picked = mixed[pl.ds(pl.multiple_of(target * rows_dev, rows_dev), rows_dev), :]
        span = slice(at * width, (at + 1) * width)
        return jnp.dot(
            picked[:, :256], out_wide[:, span], preferred_element_type=jnp.float32
        ) + jnp.dot(picked[:, 256:], out_narrow[:, span], preferred_element_type=jnp.float32)

    for at in range(columns):
        span = slice(at * width, (at + 1) * width)
        part[0, :, span] = projected(diagonal_peer, at).astype(jnp.bfloat16)
        to_partner(0, at).start()
    for at in range(columns):
        span = slice(at * width, (at + 1) * width)
        value = projected(across, at)
        to_partner(0, at).wait_recv()
        cross[:, span] = (value + part_in[0, :, span].astype(jnp.float32)).astype(jnp.bfloat16)
        to_across(at).start()
    pass_down(1)
    for at in range(columns):
        span = slice(at * width, (at + 1) * width)
        part[1, :, span] = projected(partner, at).astype(jnp.bfloat16)
        to_partner(1, at).start()
    for at in range(columns):
        span = slice(at * width, (at + 1) * width)
        value = residual[:, span].astype(jnp.float32) + projected(mine, at)
        to_partner(1, at).wait_recv()
        hidden_state[:, span] = value + part_in[1, :, span].astype(jnp.float32)
    for n in range(2, early):
        pass_down(n)
    for at in range(columns):
        to_across(at).wait_recv()
    total = hidden_state[...] + cross_in[...].astype(jnp.float32)
    hidden_state[...] = total
    scale_row = lax.rsqrt(jnp.mean(total * total, axis=-1, keepdims=True) + norm_eps)
    normed = (total * scale_row * gain[...]).astype(jnp.bfloat16)

    slot_at = lax.broadcasted_iota(jnp.int32, (capacity, rows_dev), 0).astype(jnp.float32)

    def slots(expert):
        scatter = (slot_rows[pl.ds(expert, 1), :] == slot_at).astype(jnp.bfloat16)
        return jnp.dot(scatter, normed, preferred_element_type=jnp.float32).astype(jnp.bfloat16)

    shares = 2 if capacity % 32 == 0 else 1
    share = capacity // shares

    def share_at(n):
        return pl.ds(n * share, share)

    def dispatch(expert, n):
        return remote(
            send.at[expert, share_at(n)],
            rows.at[place, mine, share_at(n)],
            z_send.at[expert, n],
            z_recv.at[place, n],
            sp=expert,
        )

    def arrived(source, n):
        return remote(
            send.at[source, share_at(n)],
            rows.at[source, mine, share_at(n)],
            z_send.at[source, n],
            z_recv.at[source, n],
            sp=source,
        )

    def forward_across(source, n):
        return remote(
            rows.at[source, mine, share_at(n)],
            rows.at[source, mine, share_at(n)],
            x_send.at[source, n],
            x_recv.at[source, n],
            tp=across,
        )

    def forward_partner(source, n):
        return remote(
            rows.at[source, mine, share_at(n)],
            rows.at[source, mine, share_at(n)],
            p_send.at[source, n],
            p_recv.at[source, n],
            tp=partner,
        )

    def pass_across(source, n):
        return remote(
            rows.at[source, across, share_at(n)],
            rows.at[source, across, share_at(n)],
            p_send.at[source, shares + n],
            p_recv.at[source, shares + n],
            tp=partner,
        )

    def forward(source, n):
        forward_across(source, n).start()
        forward_partner(source, n).start()

    def hidden_across(source):
        return remote(
            hidden_own.at[source, 1 - side],
            hidden_in.at[source, 1],
            h_send.at[source, 1],
            h_recv.at[source, 1],
            tp=across,
        )

    def hidden_partner(source):
        return remote(
            hidden_own.at[source, side],
            hidden_in.at[source, 0],
            h_send.at[source, 0],
            h_recv.at[source, 0],
            tp=partner,
        )

    def hidden_forward(source):
        return remote(
            hidden_in.at[source, 1],
            hidden_in.at[source, 2],
            h_send.at[source, 2],
            h_recv.at[source, 2],
            tp=partner,
        )

    def give_back(source):
        return remote(
            result.at[source, core],
            returned.at[place, core],
            r_send.at[source, 0],
            r_recv.at[place, core],
            sp=source,
        )

    def give_partner(source):
        return remote(
            result.at[source, 1 - core],
            returned.at[place, core],
            r_send.at[source, 1],
            r_recv.at[place, core],
            sp=source,
            tp=partner,
        )

    def came_back(expert, which):
        return remote(
            result.at[expert, 0],
            returned.at[expert, which],
            r_send.at[expert, 0],
            r_recv.at[expert, which],
            sp=expert,
        )

    @pl.loop(1, experts)
    def _(step):
        expert = peer(step)
        send[expert] = slots(expert)
        for n in range(shares):
            dispatch(expert, n).start()

    rows[place, mine] = slots(place)

    for load in loads:
        load.wait()

    ff_step = min(ff, 256)
    out_step = min(half_model, 512)

    def spread(source):
        hidden_across(source).wait_recv()
        hidden_forward(source).start()

    def finish(source):
        hidden_partner(source).wait_recv()
        hidden_forward(source).wait_recv()
        for at in range(0, half_model, out_step):
            span = slice(at, at + out_step)
            value = jnp.dot(
                hidden_own[source, side], down[0, :, span], preferred_element_type=jnp.float32
            )
            for n in range(3):
                value = value + jnp.dot(
                    hidden_in[source, n], down[n + 1, :, span], preferred_element_type=jnp.float32
                )
            value = value.astype(jnp.bfloat16)
            for n in range(2):
                result[source, n, :, span] = value[n * capacity : (n + 1) * capacity]

        @pl.when(source == place)
        def _():
            returned[place, core] = result[place, core]
            remote(
                result.at[place, 1 - core],
                returned.at[place, core],
                r_send.at[place, 1],
                r_recv.at[place, core],
                tp=partner,
            ).start()

        @pl.when(source != place)
        def _():
            give_back(source).start()
            give_partner(source).start()

    def take(step):
        later = peer(step)
        for n in range(shares):
            arrived(later, n).wait_recv()
            forward(later, n)

    def expand(source):
        for n in range(shares):
            forward_across(source, n).wait_recv()
            pass_across(source, n).start()
        for n in range(shares):
            forward_partner(source, n).wait_recv()
            pass_across(source, n).wait_recv()
        block = rows[source].reshape(4 * capacity, model_width)
        for at in range(0, ff, ff_step):
            span = slice(at, at + ff_step)
            gate_pre = jnp.dot(block, gate[:, span], preferred_element_type=jnp.float32)
            up_pre = jnp.dot(block, up[:, span], preferred_element_type=jnp.float32)
            value = activate(gate_pre, up_pre).astype(jnp.bfloat16)
            for n in range(2):
                hidden_own[source, n, :, span] = value[2 * n * capacity : 2 * (n + 1) * capacity]

    def swap_hidden(source):
        hidden_across(source).start()
        hidden_partner(source).start()

    if short:
        for n in range(early, pieces):
            down_far(n).start()
        take(1)
        take(2)
        expand(peer(1))
        for n in range(early, pieces):
            pass_down(n)
        swap_hidden(peer(1))
        expand(peer(2))
        swap_hidden(peer(2))
        take(3)
        forward(place, 0)
        down_partner.wait_recv()
        for n in range(pieces):
            down_group(n, 3 - group).wait_recv()
        spread(peer(2))
        finish(peer(2))
        spread(peer(1))
        finish(peer(1))
        expand(peer(3))
        swap_hidden(peer(3))
        for n in range(1, shares):
            forward(place, n)
        expand(place)
        swap_hidden(place)
        spread(peer(3))
        finish(peer(3))
        spread(place)
        finish(place)
    else:
        for n in range(shares):
            forward(place, n)
        take(1)
        for n in range(early, pieces):
            down_far(n).start()
        expand(place)

        @pl.loop(1, experts)
        def _(step):
            source = peer(step)
            expand(source)
            swap_hidden(source)

            @pl.when(step == 1)
            def _():
                for n in range(early, pieces):
                    pass_down(n)

            @pl.when(step + 1 < experts)
            def _():
                take(step + 1)

            @pl.when(step + 1 == experts)
            def _():
                swap_hidden(place)

            @pl.when(step == 1)
            def _():
                down_partner.wait_recv()
                for n in range(pieces):
                    down_group(n, 3 - group).wait_recv()

            spread(source)
            finish(source)

        spread(place)
        finish(place)

    slot_lane = lax.broadcasted_iota(jnp.int32, (rows_dev, capacity), 1).astype(jnp.float32)
    name_lane = lax.broadcasted_iota(jnp.int32, slot_columns.shape, 1)

    def column_of(table, expert):
        kept = jnp.where(name_lane == expert, table[...], 0.0)
        return jnp.sum(kept, axis=1, keepdims=True)

    def add_expert(expert):
        pick = (column_of(slot_columns, expert) == slot_lane).astype(jnp.bfloat16)
        weight = column_of(weight_columns, expert)
        for n in range(2):
            span = slice(n * half_model, (n + 1) * half_model)
            hidden_state[:, span] += weight * jnp.dot(
                pick, returned[expert, n], preferred_element_type=jnp.float32
            )

    came_back(place, 1 - core).wait_recv()
    add_expert(place)

    @pl.loop(1, experts)
    def _(step):
        expert = peer(step)
        came_back(expert, 0).wait_recv()
        came_back(expert, 1).wait_recv()
        add_expert(expert)

    total = hidden_state[...]
    output[...] = total.astype(output.dtype)

    @pl.loop(place + 1, experts)
    def _(target):
        send_state(place, target).wait_send()
        send_total(place, target).wait_send()

    for at in range(columns):
        to_partner(0, at).wait_send()
        to_partner(1, at).wait_send()
        to_across(at).wait_send()
    for n in range(pieces):
        down_far(n).wait_send()
        down_group(n, 2 + group).wait_send()
    down_partner.wait_send()

    @pl.loop(0, experts)
    def _(step):
        source = peer(step)
        for n in range(shares):
            forward_across(source, n).wait_send()
            forward_partner(source, n).wait_send()
            pass_across(source, n).wait_send()
        hidden_across(source).wait_send()
        hidden_partner(source).wait_send()
        hidden_forward(source).wait_send()
        give_partner(source).wait_send()

        @pl.when(step >= 1)
        def _():
            for n in range(shares):
                dispatch(source, n).wait_send()
            give_back(source).wait_send()


FINE_ROWS = 32


def rotary_tables(steps):
    grids = []
    for at in (np.arange(0, steps, FINE_ROWS), np.arange(FINE_ROWS)):
        grid = []
        for width in (HEAD_WIDE, HEAD_NARROW):
            half_width = width // 2
            inverse = np.float32(rotary_base) ** (
                -np.arange(half_width, dtype=np.float32) / np.float32(half_width)
            )
            angles = at[:, None] * np.tile(inverse.astype(np.float64), 128 // half_width)
            grid.append(np.stack([np.cos(angles), np.sin(angles)]))
        grids.append(np.stack(grid).astype(np.float32))
    return grids


def layer(mixer_inputs, decays, outs, residual, norm_gain, routes, route_weights, gate, up, down):
    experts = lax.axis_size("sp")
    rows_dev, model_width = residual.shape
    length = mixer_inputs[0].shape[0]
    ff = gate.shape[1]
    limit = max(TOP_K, 3 * rows_dev * TOP_K // (2 * experts))
    capacity = -(-limit // 16) * 16
    named = -(-experts // 8) * 8
    coarse, fine = rotary_tables(experts * length)
    bf16 = jnp.bfloat16
    block = (capacity, model_width)
    dma = pltpu.SemaphoreType.DMA
    vmem = pl.BlockSpec(memory_space=pltpu.VMEM)
    anywhere = pl.BlockSpec(memory_space=pl.ANY)
    return pl.pallas_call(
        functools.partial(tail_kernel, experts, capacity),
        out_shape=jax.ShapeDtypeStruct((rows_dev, model_width), bf16),
        in_specs=[anywhere] * 12 + [vmem] * 7,
        out_specs=vmem,
        scratch_shapes=[
            pltpu.VMEM((6, *mixer_inputs[0].shape), bf16),
            pltpu.VMEM((2, *outs[0].shape), bf16),
            pltpu.VMEM((rows_dev, model_width), bf16),
            pltpu.VMEM((model_width, ff), bf16),
            pltpu.VMEM((model_width, ff), bf16),
            pltpu.VMEM((4, ff, model_width // 2), bf16),
            pltpu.VMEM((8, length), jnp.float32),
            pltpu.VMEM((8, length), jnp.float32),
            pltpu.VMEM((length, 8), jnp.float32),
            pltpu.VMEM((2, 2, length, 128), jnp.float32),
            pltpu.VMEM((named, rows_dev), jnp.float32),
            pltpu.VMEM((rows_dev, named), jnp.float32),
            pltpu.VMEM((rows_dev, named), jnp.float32),
            pltpu.VMEM((4, rows_dev, model_width), bf16),
            pltpu.VMEM((2, rows_dev, model_width), bf16),
            pltpu.VMEM((rows_dev, model_width), bf16),
            pltpu.VMEM((rows_dev, model_width), bf16),
            pltpu.VMEM((rows_dev, model_width), jnp.float32),
            pltpu.VMEM((experts, *block), bf16),
            pltpu.VMEM((experts, 4, *block), bf16),
            pltpu.VMEM((experts, 2, 2 * capacity, ff), bf16),
            pltpu.VMEM((experts, 3, 2 * capacity, ff), bf16),
            pltpu.VMEM((experts, 2, capacity, model_width // 2), bf16),
            pltpu.VMEM((experts, 2, capacity, model_width // 2), bf16),
            pltpu.VMEM((length, 512), bf16),
            pltpu.VMEM((4, length, 128), jnp.float32),
            pltpu.VMEM((2, 4, length, 128), bf16),
            pltpu.VMEM((3, 128, 128), bf16),
            pltpu.VMEM((8, 128), jnp.float32),
            pltpu.VMEM((experts, 3, 128, 128), bf16),
            pltpu.VMEM((experts, 8, 128), jnp.float32),
            dma((12,)),
            dma((experts,)),
            dma((experts,)),
            dma((experts,)),
            dma((experts,)),
            dma((3, 4)),
            dma((3, 4)),
            dma((experts, 2)),
            dma((experts, 2)),
            dma((experts, 2)),
            dma((experts, 2)),
            dma((experts, 4)),
            dma((experts, 4)),
            dma((experts, 3)),
            dma((experts, 3)),
            dma((experts, 2)),
            dma((experts, 2)),
            dma((8,)),
            dma((8,)),
            dma((8,)),
            dma((8,)),
            dma((1,)),
            dma((1,)),
        ],
        compiler_params=pltpu.CompilerParams(
            collective_id=1, has_side_effects=True, vmem_limit_bytes=60 * 1024 * 1024
        ),
    )(
        *mixer_inputs,
        *outs,
        residual,
        gate,
        up,
        down,
        *decays,
        coarse,
        fine,
        norm_gain.reshape(1, model_width),
        routes.T,
        route_weights.T,
    )


def body(
    query_wide,
    key_wide,
    value_wide,
    decay_wide,
    query_narrow,
    key_narrow,
    value_narrow,
    decay_narrow,
    residual,
    out_wide,
    out_narrow,
    norm_gain,
    routes,
    route_weights,
    expert_gate,
    expert_up,
    expert_down,
):
    return layer(
        (
            query_wide,
            query_narrow,
            key_wide,
            key_narrow,
            value_wide,
            value_narrow,
        ),
        (decay_wide.T, decay_narrow.T),
        (out_wide, out_narrow),
        residual,
        norm_gain,
        routes,
        route_weights,
        expert_gate[0],
        expert_up[0],
        expert_down[0],
    )


def solution(mesh):
    placed = (
        P(("grp", "sp"), "tp"),
        P(("grp", "sp"), "tp"),
        P(("grp", "sp"), "tp"),
        P(("grp", "sp"), "tp"),
        P(("grp", "sp"), "tp"),
        P(("grp", "sp"), "tp"),
        P(("grp", "sp"), "tp"),
        P(("grp", "sp"), "tp"),
        P(("grp", "sp", "tp"), None),
        P("tp", None),
        P("tp", None),
        P(),
        P(("grp", "sp", "tp"), None),
        P(("grp", "sp", "tp"), None),
        P("sp", None, "tp"),
        P("sp", None, "tp"),
        P("sp", "tp", None),
    )
    return jax.shard_map(
        body, mesh=mesh, in_specs=placed, out_specs=P(("grp", "sp", "tp"), None), check_vma=False
    )
```
